512 devices in a mesh: gr: 2 (over z_hi), fs: 32 (over z_lo, y), tp: 8 (over x, core).
Axes of the slice: x: 4, y: 4, z: 16 (z_hi: 2, z_lo: 8; z = z_hi * 8 + z_lo), core: 2. Of those that a mesh axis runs over, the one named last changes fastest.
Arguments:
- tokens: bfloat16 [12288, 2048], P(('gr', 'fs')), may hold values from -6 to 6
- routes: int32 [12288, 8], P(('gr', 'fs')), may hold values from 0 to 63, all different within a row; in each aligned block of 192 rows (0 to 191, 192 to 383, ...) at most 36 rows name the same one
- route_weight: float32 [12288, 8], P(('gr', 'fs')), may hold values from 0.05 to 0.6
- norm_gain: float32 [2048], replicated, may hold values from 0.1 to 1.9
- gate_experts: float32 [2, 32, 512, 2048], P('gr', None, 'fs', 'tp'), may hold values from -0.125 to 0.125
- up_experts: float32 [2, 32, 512, 2048], P('gr', None, 'fs', 'tp'), may hold values from -0.125 to 0.125
- down_experts: float32 [2, 32, 512, 2048], P('gr', None, 'fs', 'tp'), may hold values from -0.25 to 0.25
- gate_shared: float32 [2048, 512], P('fs', 'tp'), may hold values from -0.125 to 0.125
- up_shared: float32 [2048, 512], P('fs', 'tp'), may hold values from -0.125 to 0.125
- down_shared: float32 [512, 2048], P('fs', 'tp'), may hold values from -0.25 to 0.25
Outputs:
- mixed: bfloat16 [12288, 2048], P(('gr', 'fs'), 'tp')
- gate_served: bfloat16 [2, 32, 512, 2048], P(None, 'fs', 'tp')
- up_served: bfloat16 [2, 32, 512, 2048], P(None, 'fs', 'tp')
- down_served: bfloat16 [2, 32, 512, 2048], P(None, 'fs', None, 'tp')
- gate_shared_served: bfloat16 [2048, 512], P(None, 'tp')
- up_shared_served: bfloat16 [2048, 512], P(None, 'tp')
- down_shared_served: bfloat16 [512, 2048], P(None, 'tp')
The draws below stay inside these ranges and needn't reach their ends.
Inputs may be any that keep to these rules, and one draw needn't show every extreme that they name: `routes`: each row names 8 different experts; within the 192 rows of one device no expert is named by more than 36 rows, and some expert reaches 36.
All inputs are finite; a program needn't handle non-finite values.
Results may differ from the reference program's by a relative error of at most 0.0084.
Values may be sent and summed in bfloat16 or wider, within the bound.
No kernel may reach another device: no remote copies, remote signals or barrier semaphores. Data moves between devices by JAX's collectives and lax.ppermute only.
A program may use at most 128 MiB of HBM per device.

```python
import math
import jax
import jax.numpy as jnp
import numpy as np
from jax import lax

D = 2048
DE = 512
DS = 512
TOP_K = 8
EXP_HALF = 1
TOK_DEV = 192
EXPERTS = 64
CAP = 36
TOKENS = 12288
N_GR = 2
N_FS = 32


def shard_levels(own_key, shape, pieces, low, largest):
    gain = 1.0
    for dim, shards_of in pieces:
        heights = jax.random.uniform(jax.random.fold_in(jax.random.fold_in(own_key, 6), dim), (shards_of,), jnp.float32, low / len(pieces), largest / len(pieces))
        gain = gain * jnp.repeat(jnp.exp(heights), shape[dim] // shards_of).reshape((-1,) + (1,) * (len(shape) - 1 - dim))
    return gain


def shared_out(stream_key, own, number, rows, number_of, top, most, slope):
    order = jax.random.permutation(stream_key, number_of)
    packed, ordinary = portions_of(number_of, rows * top, most, slope, True), portions_of(number_of, rows * top, most, slope, False)
    places = jnp.arange(number_of)

    def named(lengths, turn):
        used = int((lengths > 0).sum())
        fixed = max(1, used // 4)
        moved = fixed + (places - fixed + turn * (used - fixed)) % max(1, number_of - fixed)
        return jnp.zeros((number_of,), jnp.int32).at[order[jnp.where(places < fixed, places, moved)]].set(jnp.asarray(lengths, jnp.int32))

    lengths = jnp.where(number % 4 == 0, named(packed, number // 4), named(ordinary, number - number // 4 - 1))
    mixed = jax.random.permutation(jax.random.fold_in(own, 3), number_of)
    source_of, sink = mixed[0:number_of // 2 * 2:2], mixed[1:number_of // 2 * 2:2]
    margin = jnp.minimum(lengths[source_of] - 1, most - lengths[sink]) // 2
    margin = jnp.where((source_of == order[0]) | (sink == order[0]) | (lengths[sink] == 0), 0, jnp.maximum(margin, 0))
    moved = jax.random.randint(jax.random.fold_in(own, 4), (number_of // 2,), 0, 1 << 20) % (margin + 1)
    lengths = lengths.at[source_of].add(-moved).at[sink].add(moved)
    items = jnp.searchsorted(jnp.cumsum(lengths), jnp.arange(rows * top), side="right").astype(jnp.int32)
    table = items.reshape(top, rows).T
    table = table[jax.random.permutation(jax.random.fold_in(own, 1), rows)]
    turn = jax.random.randint(jax.random.fold_in(own, 2), (rows, 1), 0, top)
    return jnp.take_along_axis(table, (jnp.arange(top)[None, :] + turn) % top, axis=1)


def portions_of(amount, total, most, skew, full):
    weights = [(1 << 20) // math.isqrt(standing ** skew) + 1 for standing in range(1, amount + 1)]
    largest = most if full else min(most, max(-(-total // amount), total * weights[0] // sum(weights)))
    least = 1 if total - largest >= amount - 1 else 0
    given, surplus = [largest] + [least] * (amount - 1), total - largest - least * (amount - 1)
    while surplus > 0:
        candidates = [i for i in range(1, amount) if given[i] < largest] or [i for i in range(1, amount) if given[i] < most]
        mass, remaining = sum([weights[i] for i in candidates]), surplus
        for i in candidates:
            extra = min(most - given[i], max(1, remaining * weights[i] // mass), surplus)
            given[i] = given[i] + extra
            surplus = surplus - extra
    return np.array(given)


def normal_values(rng, dims, scale, most, pieces=(), kind=jnp.bfloat16):
    entries = scale * jax.random.normal(rng, dims, jnp.float32)
    if pieces:
        entries = entries * shard_levels(rng, dims, pieces, -0.22, 0.18)
    return jnp.clip(entries, -most, most).astype(kind)


def setup_inputs(seed: int = 0) -> dict:
    seeds = jax.random.split(jax.random.key(seed), 11)
    tokens = normal_values(seeds[0], (TOKENS, D), 1.0, 6.0, ((0, 64),))
    routes_keys = jax.random.split(jax.random.fold_in(seeds[1], 1), TOKENS // TOK_DEV)
    routes_turns = jax.random.permutation(jax.random.fold_in(seeds[1], 3), TOKENS // TOK_DEV)
    routes = jax.vmap(lambda own, number: shared_out(jax.random.fold_in(seeds[1], 2), own, number, TOK_DEV, EXPERTS, TOP_K, CAP, 1))(routes_keys, routes_turns).reshape((TOKENS, TOP_K))
    route_weight = jnp.clip(jnp.exp(math.log(0.6) - 2.4849067 * jax.random.uniform(seeds[2], (TOKENS, TOP_K), jnp.float32) ** shard_levels(seeds[2], (TOKENS, TOP_K), ((0, 64),), -0.2, 0.2)), 0.05, 0.6)
    norm_gain = jnp.clip(1.0 + 0.18 * jax.random.normal(seeds[3], (D,), jnp.float32), 0.1, 1.9)
    gate_experts = normal_values(seeds[4], (N_GR, EXP_HALF * N_FS, DE, D), D ** -0.5, 0.125, ((0, 2), (2, 32), (3, 8)), jnp.float32)
    up_experts = normal_values(seeds[5], (N_GR, EXP_HALF * N_FS, DE, D), D ** -0.5, 0.125, ((0, 2), (2, 32), (3, 8)), jnp.float32)
    down_experts = normal_values(seeds[6], (N_GR, EXP_HALF * N_FS, DE, D), DE ** -0.5, 0.25, ((0, 2), (2, 32), (3, 8)), jnp.float32)
    gate_shared = normal_values(seeds[7], (D, DS), D ** -0.5, 0.125, ((0, 32), (1, 8)), jnp.float32)
    up_shared = normal_values(seeds[8], (D, DS), D ** -0.5, 0.125, ((0, 32), (1, 8)), jnp.float32)
    down_shared = normal_values(seeds[9], (DS, D), DS ** -0.5, 0.25, ((0, 32), (1, 8)), jnp.float32)
    return dict(tokens=tokens, routes=routes, route_weight=route_weight, norm_gain=norm_gain, gate_experts=gate_experts, up_experts=up_experts, down_experts=down_experts, gate_shared=gate_shared, up_shared=up_shared, down_shared=down_shared)


EPS = 1e-06

def reference(tokens, routes, route_weight, norm_gain, gate_experts, up_experts, down_experts, gate_shared, up_shared, down_shared):
    bf = jnp.bfloat16
    f32 = jnp.float32
    gate_served = (gate_experts * norm_gain[None, None, None, :]).astype(bf)
    up_served = (up_experts * norm_gain[None, None, None, :]).astype(bf)
    down_served = down_experts.astype(bf)
    gate_sh = (gate_shared * norm_gain[:, None]).astype(bf)
    up_sh = (up_shared * norm_gain[:, None]).astype(bf)
    down_sh = down_shared.astype(bf)
    values = tokens.astype(f32)
    normed = (values * lax.rsqrt(lax.optimization_barrier(jnp.mean(values * values, axis=-1, keepdims=True)) + EPS)).astype(bf)
    count = EXPERTS
    slots_all = CAP * N_GR * N_FS
    flat_e = routes.reshape(-1).astype(jnp.int32)
    assigned = flat_e.shape[0]
    onehot = (flat_e[:, None] == jnp.arange(count, dtype=jnp.int32)[None, :]).astype(jnp.int32)
    ranks = lax.optimization_barrier(jnp.sum(jnp.cumsum(onehot, axis=0) * onehot, axis=1)) - 1
    position = (flat_e * slots_all + ranks).astype(jnp.int32)
    token_of = (jnp.arange(assigned, dtype=jnp.int32) // TOP_K).astype(jnp.int32)
    table = jnp.full((count * slots_all,), TOKENS, jnp.int32).at[position].set(token_of)
    padded = jnp.concatenate([normed, jnp.zeros((1, D), bf)], axis=0)

    def one_expert(args):
        index, w_gate, w_up, w_down = args
        rows = padded[index]
        gate = jnp.dot(rows, w_gate.T, preferred_element_type=f32)
        upper = jnp.dot(rows, w_up.T, preferred_element_type=f32)
        hidden = (jax.nn.silu(gate) * upper).astype(bf)
        return jnp.dot(hidden, w_down, preferred_element_type=f32).astype(bf)
    outputs = lax.map(one_expert, (table.reshape(count, slots_all), gate_served.reshape(count, DE, D), up_served.reshape(count, DE, D), down_served.reshape(count, DE, D)))
    picked = outputs.reshape(count * slots_all, D)[position].reshape(TOKENS, TOP_K, D)
    routed = lax.optimization_barrier(jnp.sum(picked.astype(f32) * route_weight[:, :, None], axis=1))
    shared_hidden = (jax.nn.silu(jnp.dot(normed, gate_sh, preferred_element_type=f32)) * jnp.dot(normed, up_sh, preferred_element_type=f32)).astype(bf)
    shared = jnp.dot(shared_hidden, down_sh, preferred_element_type=f32)
    mixed = (routed + shared).astype(bf)
    return (mixed, gate_served, up_served, down_served, gate_sh, up_sh, down_sh)
```

```python
import functools

import jax
import jax.numpy as jnp
from jax import lax
from jax.experimental import pallas as pl
from jax.experimental.pallas import tpu as pltpu
from jax.sharding import Mesh, PartitionSpec as P

EPS = 1e-06
bf = jnp.bfloat16
f32 = jnp.float32
FS = ("zl", "y")
TP = ("x", "core")
GF = ("gr", "zl", "y")


def slot_match(rows, experts, cap, n_fs, first, rows_dim):
    shape = (rows, experts) if rows_dim == 0 else (experts, rows)
    r = lax.broadcasted_iota(jnp.int32, shape, rows_dim) + first
    e = lax.broadcasted_iota(jnp.int32, shape, 1 - rows_dim)
    groups = experts // n_fs
    base = cap * (groups * lax.rem(e, n_fs) + lax.div(e, n_fs))
    inside = (r >= base) & (r < base + cap)
    return jnp.where(inside, 1.0, 0.0).astype(bf)


def slot_number(shape, dim, cap, first):
    r = lax.broadcasted_iota(jnp.int32, shape, dim) + first
    return lax.rem(r, cap).astype(f32)


def pack_kernel(cap, n_fs, experts, cols, chunk, at_ref, tok_ref, route_ref, weight_ref,
                normed_ref, rank_ref, mix_ref, send_ref):
    values = tok_ref[...].astype(f32)
    scale = lax.rsqrt(jnp.mean(values * values, axis=-1, keepdims=True) + EPS)
    normed_ref[...] = (values * scale).astype(bf)
    count, top = route_ref.shape
    e = lax.broadcasted_iota(jnp.int32, (count, experts), 1)
    chosen = jnp.zeros((count, experts), f32)
    mix = jnp.zeros((count, experts), f32)
    for j in range(top):
        here = route_ref[:, j : j + 1] == e
        chosen = jnp.where(here, 1.0, chosen)
        mix = jnp.where(here, weight_ref[:, j : j + 1], mix)
    row = lax.broadcasted_iota(jnp.int32, (count, count), 0)
    col = lax.broadcasted_iota(jnp.int32, (count, count), 1)
    before = jnp.where(col < row, 1.0, 0.0).astype(bf)
    rank = jnp.dot(before, chosen.astype(bf), preferred_element_type=f32)
    rank = jnp.where(chosen > 0, rank, -1.0)
    rank_ref[...] = rank
    mix_ref[...] = mix
    rank = rank.astype(bf)
    mine = normed_ref[:, pl.ds(pl.multiple_of(at_ref[0] * cols, cols), cols)]
    total = send_ref.shape[0]
    for first in range(0, total, chunk):
        owner = slot_match(chunk, experts, cap, n_fs, first, 0)
        spread = lax.dot_general(owner, rank, (((1,), (1,)), ((), ())), preferred_element_type=f32)
        pick = spread == slot_number((chunk, count), 0, cap, first)
        pick = jnp.where(pick, 1.0, 0.0).astype(bf)
        send_ref[first : first + chunk, :] = jnp.dot(pick, mine, preferred_element_type=f32).astype(bf)


def hidden_kernel(cap, n_tp, n_gr, x_ref, gate_ref, up_ref, out_ref):
    units = gate_ref.shape[1]
    cols = x_ref.shape[2]
    rows = x_ref.shape[1]
    total = jnp.zeros((2 * n_gr * units, rows), f32)
    for p in range(n_tp):
        pieces = []
        for g in range(n_gr):
            pieces.append(gate_ref[g, :, p * cols : (p + 1) * cols])
            pieces.append(up_ref[g, :, p * cols : (p + 1) * cols])
        w = jnp.concatenate(pieces, axis=0)
        total += lax.dot_general(w, x_ref[p], (((1,), (1,)), ((), ())), preferred_element_type=f32)
    slot = lax.broadcasted_iota(jnp.int32, (units, rows), 1) + pl.program_id(0) * rows
    group = lax.rem(slot, cap * n_gr) // cap
    gate, up = total[:units], total[units : 2 * units]
    for g in range(1, n_gr):
        gate = jnp.where(group == g, total[2 * g * units : (2 * g + 1) * units], gate)
        up = jnp.where(group == g, total[(2 * g + 1) * units : (2 * g + 2) * units], up)
    out_ref[...] = (gate / (1.0 + jnp.exp(-gate)) * up).astype(bf)


def mix_kernel(cap, n_fs, experts, chunk, ret_ref, rank_ref, mix_ref, shared_ref, out_ref):
    rank = rank_ref[...].astype(bf)
    high = mix_ref[...].astype(bf)
    low = (mix_ref[...] - high.astype(f32)).astype(bf)
    count = rank.shape[0]
    total = shared_ref[...]
    for first in range(0, ret_ref.shape[0], chunk):
        owner = slot_match(chunk, experts, cap, n_fs, first, 1)
        spread = jnp.dot(rank, owner, preferred_element_type=f32)
        pick = spread == slot_number((count, chunk), 1, cap, first)
        part = ret_ref[first : first + chunk, :]
        for w in (high, low):
            weight = jnp.dot(w, owner, preferred_element_type=f32)
            weight = jnp.where(pick, weight, 0.0).astype(bf)
            total += jnp.dot(weight, part, preferred_element_type=f32)
    out_ref[...] = total.astype(bf)


def spread_to(block, axis):
    copies = jnp.broadcast_to(block[None], (lax.axis_size(axis), *block.shape))
    return lax.all_to_all(copies, axis, split_axis=0, concat_axis=0, tiled=True)


def silu(v):
    return v / (1.0 + jnp.exp(-v))


def on_device(tokens, routes, route_weight, norm_gain, gate_experts, up_experts, down_experts,
              gate_shared, up_shared, down_shared):
    n_gr, n_fs, n_tp = lax.axis_size("gr"), lax.axis_size(FS), lax.axis_size(TP)
    n_z, n_y = lax.axis_size("zl"), lax.axis_size("y")
    n_x = lax.axis_size("x")
    fs_at, tp_at, core = lax.axis_index(FS), lax.axis_index(TP), lax.axis_index("core")
    per_group, rows_here, cols = gate_experts.shape[1:]
    count, top = routes.shape
    width = tokens.shape[1]
    experts = per_group * n_gr
    cap = (3 * count * top + 2 * experts - 1) // (2 * experts)
    slots = experts * cap

    vmem = pltpu.CompilerParams(vmem_limit_bytes=48 * 1024 * 1024)
    normed, rank, mix, send = pl.pallas_call(
        functools.partial(pack_kernel, cap, n_fs, experts, cols, slots // 8),
        out_shape=(
            jax.ShapeDtypeStruct((count, width), bf),
            jax.ShapeDtypeStruct((count, experts), f32),
            jax.ShapeDtypeStruct((count, experts), f32),
            jax.ShapeDtypeStruct((slots, cols), bf),
        ),
        in_specs=[pl.BlockSpec(memory_space=pltpu.SMEM)] + [pl.BlockSpec(memory_space=pltpu.VMEM)] * 3,
        out_specs=(pl.BlockSpec(memory_space=pltpu.VMEM),) * 4,
        compiler_params=vmem,
        name="pack",
    )(tp_at.astype(jnp.int32).reshape(1), tokens, routes, route_weight)
    received = lax.all_to_all(send, FS, split_axis=0, concat_axis=0, tiled=True)
    rows_all = lax.all_gather(received, TP, axis=0, tiled=True).reshape(n_tp, slots, cols)

    gain = lax.dynamic_slice_in_dim(norm_gain, tp_at * cols, cols, 0)
    gate_local = (gate_experts[0] * gain).astype(bf)
    up_local = (up_experts[0] * gain).astype(bf)
    both = jnp.stack([gate_local, up_local], axis=1)
    both = jnp.broadcast_to(both[None], (n_gr, *both.shape)).reshape(n_gr * per_group, 2, rows_here, cols)
    both = lax.all_to_all(both, GF, split_axis=0, concat_axis=0, tiled=True)
    down_local = down_experts[0].astype(bf)
    down_all = jnp.broadcast_to(down_local[None], (n_gr, *down_local.shape)).reshape(-1, rows_here, cols)
    down_all = lax.all_to_all(down_all, GF, split_axis=0, concat_axis=0, tiled=True)
    down_w = down_all.reshape(n_gr, n_fs * rows_here, cols)

    near = n_fs // n_tp
    both = both.reshape(n_gr, n_tp, near, 2, rows_here, cols).transpose(1, 3, 0, 2, 4, 5)
    both = lax.all_to_all(both, TP, split_axis=0, concat_axis=0, tiled=True)
    units = near * rows_here
    both = both.reshape(n_tp, 2, n_gr, units, cols).transpose(1, 2, 3, 0, 4)
    gate_w, up_w = both[0].reshape(n_gr, units, width), both[1].reshape(n_gr, units, width)

    sh_rows, sh_cols = gate_shared.shape
    gain_sh = lax.dynamic_slice_in_dim(norm_gain, fs_at * sh_rows, sh_rows, 0)[:, None]
    pair = jnp.concatenate([(gate_shared * gain_sh).astype(bf), (up_shared * gain_sh).astype(bf)], axis=1)
    half = sh_rows * 2 * sh_cols // cols
    times = sh_rows // half
    pair = jnp.concatenate([pair[i * half : (i + 1) * half] for i in range(times)], axis=1)
    block = jnp.concatenate([pair, down_shared.astype(bf)], axis=0)
    block = spread_to(block, "zl")
    block = spread_to(block, "y")
    block = block.reshape(n_y, n_z, half + down_shared.shape[0], cols).transpose(1, 0, 2, 3)
    pair = block[:, :, :half].reshape(n_fs, half, times, 2 * sh_cols).transpose(0, 2, 1, 3)
    pair = pair.reshape(width, 2 * sh_cols)
    gate_sw, up_sw = pair[:, :sh_cols], pair[:, sh_cols:]
    down_sw = block[:, :, half:].reshape(-1, cols)

    turned = lax.dot_general(pair, normed, (((0,), (1,)), ((), ())), preferred_element_type=f32)
    shared_hidden = (silu(turned[:sh_cols]) * turned[sh_cols:]).astype(bf)

    row_block = slots // 6
    hidden = pl.pallas_call(
        functools.partial(hidden_kernel, cap, n_tp, n_gr),
        out_shape=jax.ShapeDtypeStruct((units, slots), bf),
        grid=(slots // row_block,),
        in_specs=[
            pl.BlockSpec((n_tp, row_block, cols), lambda i: (0, i, 0)),
            pl.BlockSpec((n_gr, units, width), lambda i: (0, 0, 0)),
            pl.BlockSpec((n_gr, units, width), lambda i: (0, 0, 0)),
        ],
        out_specs=pl.BlockSpec((units, row_block), lambda i: (0, i)),
        compiler_params=vmem,
        cost_estimate=pl.CostEstimate(
            flops=4 * n_gr * units * slots * width, bytes_accessed=2 * slots * width, transcendentals=units * slots
        ),
        name="gate_up",
    )(rows_all, gate_w, up_w)
    hidden = jnp.concatenate([hidden, shared_hidden], axis=1)
    near_hidden = spread_to(hidden, "x").reshape(n_x * units, slots + count)
    far_hidden = lax.ppermute(near_hidden, "core", [(0, 1), (1, 0)])

    def part(w, which):
        w = w.reshape(n_x, 2, units, *w.shape[1:])
        return lax.dynamic_index_in_dim(w, which, 1, keepdims=False).reshape(n_x * units, -1)

    def applied(lo, hi, w):
        turn = (((0,), (0,)), ((), ()))
        out = lax.dot_general(near_hidden[:, lo:hi], part(w, core), turn, preferred_element_type=f32)
        return out + lax.dot_general(far_hidden[:, lo:hi], part(w, 1 - core), turn, preferred_element_type=f32)

    down_cat = jnp.concatenate([down_w[g] for g in range(n_gr)], axis=1)
    result = applied(0, slots, down_cat)
    group = lax.rem(lax.broadcasted_iota(jnp.int32, (slots, cols), 0), cap * n_gr) // cap
    picked = result[:, :cols]
    for g in range(1, n_gr):
        picked = jnp.where(group == g, result[:, g * cols : (g + 1) * cols], picked)
    returned = lax.all_to_all(picked.astype(bf), FS, split_axis=0, concat_axis=0, tiled=True)
    shared = applied(slots, slots + count, down_sw)
    mixed = pl.pallas_call(
        functools.partial(mix_kernel, cap, n_fs, experts, slots // 6),
        out_shape=jax.ShapeDtypeStruct((count, cols), bf),
        in_specs=[pl.BlockSpec(memory_space=pltpu.VMEM)] * 4,
        out_specs=pl.BlockSpec(memory_space=pltpu.VMEM),
        compiler_params=vmem,
        name="mix",
    )(returned, rank, mix, shared)
    return (mixed, gate_w[:, None], up_w[:, None], down_w[:, None], gate_sw, up_sw, down_sw)


def solution(mesh):
    gr, fs, tp = mesh.devices.shape
    n_y = 4 if fs % 4 == 0 else 1
    fine = Mesh(mesh.devices.reshape(gr, fs // n_y, n_y, tp // 2, 2), ("gr", "zl", "y", "x", "core"))
    return jax.shard_map(
        on_device,
        mesh=fine,
        in_specs=(
            P(GF, None),
            P(GF, None),
            P(GF, None),
            P(),
            P("gr", None, FS, TP),
            P("gr", None, FS, TP),
            P("gr", None, FS, TP),
            P(FS, TP),
            P(FS, TP),
            P(FS, TP),
        ),
        out_specs=(
            P(GF, TP),
            P(None, FS, TP, None),
            P(None, FS, TP, None),
            P(None, FS, None, TP),
            P(None, TP),
            P(None, TP),
            P(None, TP),
        ),
        check_vma=False,
    )
```

```python
import functools

import jax
import jax.numpy as jnp
from jax import lax
from jax.experimental import pallas as pl
from jax.experimental.pallas import tpu as pltpu
from jax.sharding import Mesh, PartitionSpec as P

EPS = 1e-06
bf = jnp.bfloat16
f32 = jnp.float32
FS = ("zl", "y")
TP = ("x", "core")
GF = ("gr", "zl", "y")


def slot_match(rows, experts, cap, n_fs, first, rows_dim):
    shape = (rows, experts) if rows_dim == 0 else (experts, rows)
    r = lax.broadcasted_iota(jnp.int32, shape, rows_dim) + first
    e = lax.broadcasted_iota(jnp.int32, shape, 1 - rows_dim)
    groups = experts // n_fs
    base = cap * (groups * lax.rem(e, n_fs) + lax.div(e, n_fs))
    inside = (r >= base) & (r < base + cap)
    return jnp.where(inside, 1.0, 0.0).astype(bf)


def slot_number(shape, dim, cap, first):
    r = lax.broadcasted_iota(jnp.int32, shape, dim) + first
    return lax.rem(r, cap).astype(f32)


def pack_kernel(cap, n_fs, experts, cols, chunk, at_ref, tok_ref, route_ref, weight_ref,
                normed_ref, rank_ref, mix_ref, send_ref):
    values = tok_ref[...].astype(f32)
    scale = lax.rsqrt(jnp.mean(values * values, axis=-1, keepdims=True) + EPS)
    normed_ref[...] = (values * scale).astype(bf)
    count, top = route_ref.shape
    e = lax.broadcasted_iota(jnp.int32, (count, experts), 1)
    chosen = jnp.zeros((count, experts), f32)
    mix = jnp.zeros((count, experts), f32)
    for j in range(top):
        here = route_ref[:, j : j + 1] == e
        chosen = jnp.where(here, 1.0, chosen)
        mix = jnp.where(here, weight_ref[:, j : j + 1], mix)
    row = lax.broadcasted_iota(jnp.int32, (count, count), 0)
    col = lax.broadcasted_iota(jnp.int32, (count, count), 1)
    before = jnp.where(col < row, 1.0, 0.0).astype(bf)
    rank = jnp.dot(before, chosen.astype(bf), preferred_element_type=f32)
    rank = jnp.where(chosen > 0, rank, -1.0)
    rank_ref[...] = rank
    mix_ref[...] = mix
    rank = rank.astype(bf)
    mine = normed_ref[:, pl.ds(pl.multiple_of(at_ref[0] * cols, cols), cols)]
    total = send_ref.shape[0]
    for first in range(0, total, chunk):
        owner = slot_match(chunk, experts, cap, n_fs, first, 0)
        spread = lax.dot_general(owner, rank, (((1,), (1,)), ((), ())), preferred_element_type=f32)
        pick = spread == slot_number((chunk, count), 0, cap, first)
        pick = jnp.where(pick, 1.0, 0.0).astype(bf)
        send_ref[first : first + chunk, :] = jnp.dot(pick, mine, preferred_element_type=f32).astype(bf)


def hidden_kernel(cap, n_gr, at_ref, x_ref, shared_ref, *refs):
    n_tp = x_ref.shape[0]
    pieces, (out_ref, gate_ref, up_ref, w_ref) = refs[:n_tp], refs[n_tp:]
    near, rows_here, cols = pieces[0].shape[1], pieces[0].shape[3], pieces[0].shape[4]
    units = near * rows_here
    rows = x_ref.shape[1]

    @pl.when(pl.program_id(0) == 0)
    def _():
        for j in range(n_tp):
            owner = lax.rem(at_ref[0] + j, n_tp)
            lanes = pl.ds(pl.multiple_of(owner * cols, cols), cols)
            for g in range(n_gr):
                for q in range(near):
                    for mat, served in ((0, gate_ref), (1, up_ref)):
                        piece = pieces[j][g, q, mat]
                        first = q * rows_here
                        served[g, first : first + rows_here, lanes] = piece
                        first += (2 * g + mat) * units
                        w_ref[first : first + rows_here, lanes] = piece
        out_ref[:, out_ref.shape[1] - shared_ref.shape[1] :] = shared_ref[...]

    total = jnp.zeros((2 * n_gr * units, rows), f32)
    for p in range(n_tp):
        w = w_ref[:, p * cols : (p + 1) * cols]
        total += lax.dot_general(w, x_ref[p], (((1,), (1,)), ((), ())), preferred_element_type=f32)
    slot = lax.broadcasted_iota(jnp.int32, (units, rows), 1) + pl.program_id(0) * rows
    group = lax.div(lax.rem(slot, cap * n_gr), cap)
    gate, up = total[:units], total[units : 2 * units]
    for g in range(1, n_gr):
        gate = jnp.where(group == g, total[2 * g * units : (2 * g + 1) * units], gate)
        up = jnp.where(group == g, total[(2 * g + 1) * units : (2 * g + 2) * units], up)
    hidden = (gate / (1.0 + jnp.exp(-gate)) * up).astype(bf)
    out_ref[:, pl.ds(pl.multiple_of(pl.program_id(0) * rows, 128), rows)] = hidden


def down_kernel(cap, n_gr, chunk, at_ref, down_ref, down_sh_ref, *refs):
    pieces, (out_ref, shared_ref, h_ref) = refs[:-3], refs[-3:]
    n_x = len(pieces) // 2
    units = pieces[0].shape[0]
    cols = out_ref.shape[1]
    for c in range(2):
        core = at_ref[1] if c == 0 else 1 - at_ref[1]
        for j in range(n_x):
            first = (lax.rem(at_ref[0] + j, n_x) * 2 + core) * units
            h_ref[pl.ds(pl.multiple_of(first, units), units), :] = pieces[c * n_x + j][...]
    turn = (((0,), (0,)), ((), ()))
    slots = out_ref.shape[0]
    for first in range(0, slots, chunk):
        h = h_ref[:, first : first + chunk]
        slot = lax.broadcasted_iota(jnp.int32, (chunk, cols), 0) + first
        group = lax.div(lax.rem(slot, cap * n_gr), cap)
        picked = lax.dot_general(h, down_ref[0], turn, preferred_element_type=f32)
        for g in range(1, n_gr):
            other = lax.dot_general(h, down_ref[g], turn, preferred_element_type=f32)
            picked = jnp.where(group == g, other, picked)
        out_ref[first : first + chunk, :] = picked.astype(bf)
    shared_ref[...] = lax.dot_general(h_ref[:, slots:], down_sh_ref[...], turn, preferred_element_type=f32)


def mix_kernel(cap, n_fs, experts, chunk, ret_ref, rank_ref, mix_ref, shared_ref, out_ref):
    rank = rank_ref[...].astype(bf)
    high = mix_ref[...].astype(bf)
    low = (mix_ref[...] - high.astype(f32)).astype(bf)
    count = rank.shape[0]
    total = shared_ref[...]
    for first in range(0, ret_ref.shape[0], chunk):
        owner = slot_match(chunk, experts, cap, n_fs, first, 1)
        spread = jnp.dot(rank, owner, preferred_element_type=f32)
        pick = spread == slot_number((count, chunk), 1, cap, first)
        part = ret_ref[first : first + chunk, :]
        for w in (high, low):
            weight = jnp.dot(w, owner, preferred_element_type=f32)
            weight = jnp.where(pick, weight, 0.0).astype(bf)
            total += jnp.dot(weight, part, preferred_element_type=f32)
    out_ref[...] = total.astype(bf)


def silu(v):
    return v / (1.0 + jnp.exp(-v))


def on_device(tokens, routes, route_weight, norm_gain, gate_experts, up_experts, down_experts,
              gate_shared, up_shared, down_shared):
    n_gr, n_fs, n_tp = lax.axis_size("gr"), lax.axis_size(FS), lax.axis_size(TP)
    n_x = lax.axis_size("x")
    fs_at, tp_at, core = lax.axis_index(FS), lax.axis_index(TP), lax.axis_index("core")
    per_group, rows_here, cols = gate_experts.shape[1:]
    count, top = routes.shape
    width = tokens.shape[1]
    experts = per_group * n_gr
    cap = (3 * count * top + 2 * experts - 1) // (2 * experts)
    slots = experts * cap

    vmem = pltpu.CompilerParams(vmem_limit_bytes=48 * 1024 * 1024)
    normed, rank, mix, send = pl.pallas_call(
        functools.partial(pack_kernel, cap, n_fs, experts, cols, slots // 8),
        out_shape=(
            jax.ShapeDtypeStruct((count, width), bf),
            jax.ShapeDtypeStruct((count, experts), f32),
            jax.ShapeDtypeStruct((count, experts), f32),
            jax.ShapeDtypeStruct((slots, cols), bf),
        ),
        in_specs=[pl.BlockSpec(memory_space=pltpu.SMEM)] + [pl.BlockSpec(memory_space=pltpu.VMEM)] * 3,
        out_specs=(pl.BlockSpec(memory_space=pltpu.VMEM),) * 4,
        compiler_params=vmem,
        name="pack",
    )(tp_at.astype(jnp.int32).reshape(1), tokens, routes, route_weight)
    received = lax.all_to_all(send, FS, split_axis=0, concat_axis=0, tiled=True)
    rows_all = lax.all_gather(received, TP, axis=0, tiled=True).reshape(n_tp, slots, cols)

    gain = lax.dynamic_slice_in_dim(norm_gain, tp_at * cols, cols, 0)
    gate_local = (gate_experts[0] * gain).astype(bf)
    up_local = (up_experts[0] * gain).astype(bf)
    both = jnp.stack([gate_local, up_local], axis=1)
    both = jnp.broadcast_to(both[None], (n_gr, *both.shape)).reshape(n_gr * per_group, 2, rows_here, cols)
    both = lax.all_to_all(both, GF, split_axis=0, concat_axis=0, tiled=True)
    down_local = down_experts[0].astype(bf)
    down_all = jnp.broadcast_to(down_local[None], (n_gr, *down_local.shape)).reshape(-1, rows_here, cols)
    down_all = lax.all_to_all(down_all, GF, split_axis=0, concat_axis=0, tiled=True)
    down_w = down_all.reshape(n_gr, n_fs * rows_here, cols)

    near = n_fs // n_tp
    units = near * rows_here
    both = both.reshape(n_gr, n_tp, near, 2, rows_here, cols)

    def for_device(p):
        return lax.dynamic_index_in_dim(both, lax.rem(p, n_tp), 1, keepdims=False)

    pieces = [for_device(tp_at)]
    for j in range(1, n_tp):
        d = n_tp - j
        pieces.append(lax.ppermute(for_device(tp_at + d), TP, [(i, (i + d) % n_tp) for i in range(n_tp)]))

    sh_rows, sh_cols = gate_shared.shape
    gain_sh = lax.dynamic_slice_in_dim(norm_gain, fs_at * sh_rows, sh_rows, 0)[:, None]
    pair = jnp.concatenate([(gate_shared * gain_sh).astype(bf), (up_shared * gain_sh).astype(bf)], axis=1)
    half = sh_rows * 2 * sh_cols // cols
    times = sh_rows // half
    pair = jnp.concatenate([pair[i * half : (i + 1) * half] for i in range(times)], axis=1)
    block = jnp.concatenate([pair, down_shared.astype(bf)], axis=0)
    block = lax.all_gather(block, GF, axis=0)[:n_fs]
    pair = block[:, :half].reshape(n_fs, half, times, 2 * sh_cols).transpose(0, 2, 1, 3)
    pair = pair.reshape(width, 2 * sh_cols)
    gate_sw, up_sw = pair[:, :sh_cols], pair[:, sh_cols:]
    down_sw = block[:, half:].reshape(-1, cols)

    turned = lax.dot_general(pair, normed, (((0,), (1,)), ((), ())), preferred_element_type=f32)
    shared_hidden = (silu(turned[:sh_cols]) * turned[sh_cols:]).astype(bf)

    row_block = slots // 6
    in_smem, in_vmem = pl.BlockSpec(memory_space=pltpu.SMEM), pl.BlockSpec(memory_space=pltpu.VMEM)
    whole = pl.BlockSpec((n_gr, units, width), lambda i: (0, 0, 0))
    hidden, gate_w, up_w = pl.pallas_call(
        functools.partial(hidden_kernel, cap, n_gr),
        out_shape=(
            jax.ShapeDtypeStruct((units, slots + count), bf),
            jax.ShapeDtypeStruct((n_gr, units, width), bf),
            jax.ShapeDtypeStruct((n_gr, units, width), bf),
        ),
        grid=(slots // row_block,),
        in_specs=[in_smem, pl.BlockSpec((n_tp, row_block, cols), lambda i: (0, i, 0))] + [in_vmem] * (1 + n_tp),
        out_specs=(pl.BlockSpec((units, slots + count), lambda i: (0, 0)), whole, whole),
        scratch_shapes=[pltpu.VMEM((2 * n_gr * units, width), bf)],
        compiler_params=vmem,
        cost_estimate=pl.CostEstimate(
            flops=4 * n_gr * units * slots * width, bytes_accessed=2 * slots * width, transcendentals=units * slots
        ),
        name="gate_up",
    )(tp_at.astype(jnp.int32).reshape(1), rows_all, shared_hidden, *pieces)
    mine = [hidden]
    for j in range(1, n_x):
        d = n_x - j
        mine.append(lax.ppermute(hidden, "x", [(i, (i + d) % n_x) for i in range(n_x)]))
    others = [lax.ppermute(h, "core", [(0, 1), (1, 0)]) for h in mine]
    place = jnp.stack([lax.axis_index("x"), core]).astype(jnp.int32)
    picked, shared = pl.pallas_call(
        functools.partial(down_kernel, cap, n_gr, row_block),
        out_shape=(jax.ShapeDtypeStruct((slots, cols), bf), jax.ShapeDtypeStruct((count, cols), f32)),
        in_specs=[in_smem] + [in_vmem] * (2 + 2 * n_x),
        out_specs=(in_vmem, in_vmem),
        scratch_shapes=[pltpu.VMEM((n_tp * units, slots + count), bf)],
        compiler_params=vmem,
        cost_estimate=pl.CostEstimate(
            flops=2 * n_gr * slots * n_tp * units * cols, bytes_accessed=2 * slots * n_tp * units, transcendentals=0
        ),
        name="down",
    )(place, down_w, down_sw, *mine, *others)
    returned = lax.all_to_all(picked, FS, split_axis=0, concat_axis=0, tiled=True)
    mixed = pl.pallas_call(
        functools.partial(mix_kernel, cap, n_fs, experts, slots // 6),
        out_shape=jax.ShapeDtypeStruct((count, cols), bf),
        in_specs=[pl.BlockSpec(memory_space=pltpu.VMEM)] * 4,
        out_specs=pl.BlockSpec(memory_space=pltpu.VMEM),
        compiler_params=vmem,
        name="mix",
    )(returned, rank, mix, shared)
    return (mixed, gate_w[:, None], up_w[:, None], down_w[:, None], gate_sw, up_sw, down_sw)


def solution(mesh):
    gr, fs, tp = mesh.devices.shape
    n_y = 4 if fs % 4 == 0 else 1
    fine = Mesh(mesh.devices.reshape(gr, fs // n_y, n_y, tp // 2, 2), ("gr", "zl", "y", "x", "core"))
    return jax.shard_map(
        on_device,
        mesh=fine,
        in_specs=(
            P(GF, None),
            P(GF, None),
            P(GF, None),
            P(),
            P("gr", None, FS, TP),
            P("gr", None, FS, TP),
            P("gr", None, FS, TP),
            P(FS, TP),
            P(FS, TP),
            P(FS, TP),
        ),
        out_specs=(
            P(GF, TP),
            P(None, FS, TP, None),
            P(None, FS, TP, None),
            P(None, FS, None, TP),
            P(None, TP),
            P(None, TP),
            P(None, TP),
        ),
        check_vma=False,
    )
```

```python
import functools

import jax
import jax.numpy as jnp
from jax import lax
from jax.experimental import pallas as pl
from jax.experimental.pallas import tpu as pltpu
from jax.sharding import Mesh, PartitionSpec as P

EPS = 1e-06
bf = jnp.bfloat16
f32 = jnp.float32
FS = ("zl", "y")
TP = ("x", "core")
GF = ("gr", "zl", "y")


def slot_match(at_ref, rows, experts, cap, n_z, n_y, first, rows_dim):
    shape = (rows, experts) if rows_dim == 0 else (experts, rows)
    r = lax.broadcasted_iota(jnp.int32, shape, rows_dim) + first
    e = lax.broadcasted_iota(jnp.int32, shape, 1 - rows_dim)
    groups = experts // (n_z * n_y)
    k = lax.rem(e, n_z * n_y)
    z_off = lax.rem(lax.div(k, n_y) - at_ref[1] + n_z, n_z)
    y_off = lax.rem(lax.rem(k, n_y) - at_ref[2] + n_y, n_y)
    base = cap * (groups * (z_off * n_y + y_off) + lax.div(e, n_z * n_y))
    inside = (r >= base) & (r < base + cap)
    return jnp.where(inside, 1.0, 0.0).astype(bf)


def slot_number(shape, dim, cap):
    return lax.rem(lax.broadcasted_iota(jnp.int32, shape, dim), cap).astype(f32)


def pack_kernel(cap, n_z, n_y, experts, cols, at_ref, tok_ref, route_ref, weight_ref,
                normed_ref, rank_ref, mix_ref, *send_refs):
    values = tok_ref[...].astype(f32)
    scale = lax.rsqrt(jnp.mean(values * values, axis=-1, keepdims=True) + EPS)
    normed_ref[...] = (values * scale).astype(bf)
    count, top = route_ref.shape
    e = lax.broadcasted_iota(jnp.int32, (count, experts), 1)
    chosen = jnp.zeros((count, experts), f32)
    mix = jnp.zeros((count, experts), f32)
    for j in range(top):
        here = route_ref[:, j : j + 1] == e
        chosen = jnp.where(here, 1.0, chosen)
        mix = jnp.where(here, weight_ref[:, j : j + 1], mix)
    row = lax.broadcasted_iota(jnp.int32, (count, count), 0)
    col = lax.broadcasted_iota(jnp.int32, (count, count), 1)
    before = jnp.where(col < row, 1.0, 0.0).astype(bf)
    rank = jnp.dot(before, chosen.astype(bf), preferred_element_type=f32)
    rank = jnp.where(chosen > 0, rank, -1.0)
    rank_ref[...] = rank
    mix_ref[...] = mix
    rank = rank.astype(bf)
    mine = normed_ref[:, pl.ds(pl.multiple_of(at_ref[0] * cols, cols), cols)]
    chunk = send_refs[0].shape[0]
    number = slot_number((chunk, count), 0, cap)
    for i, send_ref in enumerate(send_refs):
        owner = slot_match(at_ref, chunk, experts, cap, n_z, n_y, i * chunk, 0)
        spread = lax.dot_general(owner, rank, (((1,), (1,)), ((), ())), preferred_element_type=f32)
        pick = jnp.where(spread == number, 1.0, 0.0).astype(bf)
        send_ref[...] = jnp.dot(pick, mine, preferred_element_type=f32).astype(bf)


def shared_kernel(n_z, n_y, half, times, at_ref, block_ref, normed_ref,
                  gate_ref, up_ref, down_ref, hidden_ref, pair_ref):
    rows = half * times
    both = pair_ref.shape[1]
    below = block_ref.shape[1] - half
    for p in range(n_z * n_y):
        z, y = p // n_y, p % n_y
        here = jnp.bitwise_xor(at_ref[1], z) + n_z * jnp.bitwise_xor(at_ref[2], y)
        for i in range(times):
            first = p * rows + i * half
            pair_ref[first : first + half, :] = block_ref[here, :half, i * both : (i + 1) * both]
        down_ref[p * below : (p + 1) * below, :] = block_ref[here, half:, :]
    pair = pair_ref[...]
    gate_ref[...] = pair[:, : both // 2]
    up_ref[...] = pair[:, both // 2 :]
    turned = jnp.dot(normed_ref[...], pair, preferred_element_type=f32).T
    gate, up = turned[: both // 2], turned[both // 2 :]
    hidden_ref[...] = (gate / (1.0 + jnp.exp(-gate)) * up).astype(bf)


def hidden_kernel(cap, n_gr, at_ref, shared_ref, *refs):
    n_x = (len(refs) - 4) // 3
    rows_refs, pieces, (out_ref, gate_ref, up_ref, w_ref) = refs[: 2 * n_x], refs[2 * n_x : 3 * n_x], refs[3 * n_x :]
    near, rows_here, cols = pieces[0].shape[2], pieces[0].shape[4], pieces[0].shape[5]
    units = near * rows_here
    rows = rows_refs[0].shape[0]

    def lanes_of(c, j):
        core = at_ref[4] if c == 0 else 1 - at_ref[4]
        owner = lax.rem(at_ref[3] + j, n_x) * 2 + core
        return pl.ds(pl.multiple_of(owner * cols, cols), cols)

    @pl.when(pl.program_id(0) == 0)
    def _():
        for j in range(n_x):
            for c in range(2):
                lanes = lanes_of(c, j)
                for g in range(n_gr):
                    for q in range(near):
                        for mat, served in ((0, gate_ref), (1, up_ref)):
                            piece = pieces[j][c, g, q, mat]
                            first = q * rows_here
                            served[g, first : first + rows_here, lanes] = piece
                            first += (2 * g + mat) * units
                            w_ref[first : first + rows_here, lanes] = piece
        out_ref[:, out_ref.shape[1] - shared_ref.shape[1] :] = shared_ref[...]

    total = jnp.zeros((2 * n_gr * units, rows), f32)
    for j in range(n_x):
        for c in range(2):
            w = w_ref[:, lanes_of(c, j)]
            total += lax.dot_general(
                w, rows_refs[c * n_x + j][...], (((1,), (1,)), ((), ())), preferred_element_type=f32
            )
    slot = lax.broadcasted_iota(jnp.int32, (units, rows), 1) + pl.program_id(0) * rows
    group = lax.div(lax.rem(slot, cap * n_gr), cap)
    gate, up = total[:units], total[units : 2 * units]
    for g in range(1, n_gr):
        gate = jnp.where(group == g, total[2 * g * units : (2 * g + 1) * units], gate)
        up = jnp.where(group == g, total[(2 * g + 1) * units : (2 * g + 2) * units], up)
    hidden = (gate / (1.0 + jnp.exp(-gate)) * up).astype(bf)
    out_ref[:, pl.ds(pl.multiple_of(pl.program_id(0) * rows, 128), rows)] = hidden


def down_kernel(cap, n_gr, n_y, at_ref, down_ref, down_sh_ref, *refs):
    pieces, outs, (shared_ref, h_ref) = refs[: -2 - n_y], refs[-2 - n_y : -2], refs[-2:]
    n_x = len(pieces) // 2
    units = pieces[0].shape[0]
    each, cols = outs[0].shape
    for c in range(2):
        core = at_ref[4] if c == 0 else 1 - at_ref[4]
        for j in range(n_x):
            first = (lax.rem(at_ref[3] + j, n_x) * 2 + core) * units
            h_ref[pl.ds(pl.multiple_of(first, units), units), :] = pieces[c * n_x + j][...]
    turn = (((0,), (0,)), ((), ()))
    for pair in range(n_y // 2):
        first = pair * 2 * each
        h = h_ref[:, first : first + 2 * each]
        slot = lax.broadcasted_iota(jnp.int32, (2 * each, cols), 0) + first
        group = lax.div(lax.rem(slot, cap * n_gr), cap)
        picked = lax.dot_general(h, down_ref[0], turn, preferred_element_type=f32)
        for g in range(1, n_gr):
            other = lax.dot_general(h, down_ref[g], turn, preferred_element_type=f32)
            picked = jnp.where(group == g, other, picked)
        picked = picked.astype(bf)
        outs[2 * pair][...] = picked[:each]
        outs[2 * pair + 1][...] = picked[each:]
    slots = n_y * each
    shared_ref[...] = lax.dot_general(h_ref[:, slots:], down_sh_ref[...], turn, preferred_element_type=f32)


def mix_kernel(cap, n_z, n_y, experts, at_ref, rank_ref, mix_ref, shared_ref, *refs):
    parts, out_ref = refs[:-1], refs[-1]
    rank = rank_ref[...].astype(bf)
    high = mix_ref[...].astype(bf)
    low = (mix_ref[...] - high.astype(f32)).astype(bf)
    count = rank.shape[0]
    total = shared_ref[...]
    chunk = parts[0].shape[0]
    number = slot_number((count, chunk), 1, cap)
    for i, part_ref in enumerate(parts):
        owner = slot_match(at_ref, chunk, experts, cap, n_z, n_y, i * chunk, 1)
        pick = jnp.dot(rank, owner, preferred_element_type=f32) == number
        part = part_ref[...]
        for w in (high, low):
            weight = jnp.dot(w, owner, preferred_element_type=f32)
            weight = jnp.where(pick, weight, 0.0).astype(bf)
            total += jnp.dot(weight, part, preferred_element_type=f32)
    out_ref[...] = total.astype(bf)


def turned_by(value, axis, d):
    n = lax.axis_size(axis)
    return lax.ppermute(value, axis, [(i, (i + d) % n) for i in range(n)]) if d % n else value


def crossed_with(value, axis, bit):
    return lax.ppermute(value, axis, [(i, i ^ bit) for i in range(lax.axis_size(axis))])


def along_z(value, z_off, back):
    n_gr, n_z, n_y = lax.axis_size("gr"), lax.axis_size("zl"), lax.axis_size("y")
    if z_off == 0:
        return value
    pairs = []
    for z in range(n_gr * n_z):
        for y in range(n_y):
            near = 2 * z_off < n_z or (2 * z_off == n_z and y % 2 == 0)
            other = (z + (z_off if near else z_off - n_z)) % (n_gr * n_z)
            pair = (z * n_y + y, other * n_y + y)
            pairs.append(pair[::-1] if back else pair)
    return lax.ppermute(value, GF, pairs)


def on_device(tokens, routes, route_weight, norm_gain, gate_experts, up_experts, down_experts,
              gate_shared, up_shared, down_shared):
    n_gr, n_fs, n_tp = lax.axis_size("gr"), lax.axis_size(FS), lax.axis_size(TP)
    n_z, n_y, n_x = lax.axis_size("zl"), lax.axis_size("y"), lax.axis_size("x")
    fs_at, tp_at, x_at, core = lax.axis_index(FS), lax.axis_index(TP), lax.axis_index("x"), lax.axis_index("core")
    at = jnp.stack([tp_at, lax.axis_index("zl"), lax.axis_index("y"), x_at, core]).astype(jnp.int32)
    per_group, rows_here, cols = gate_experts.shape[1:]
    count, top = routes.shape
    width = tokens.shape[1]
    experts = per_group * n_gr
    cap = (3 * count * top + 2 * experts - 1) // (2 * experts)
    slots = experts * cap
    block_rows = n_gr * cap

    in_smem, in_vmem = pl.BlockSpec(memory_space=pltpu.SMEM), pl.BlockSpec(memory_space=pltpu.VMEM)
    vmem = pltpu.CompilerParams(vmem_limit_bytes=48 * 1024 * 1024)
    normed, rank, mix, *send = pl.pallas_call(
        functools.partial(pack_kernel, cap, n_z, n_y, experts, cols),
        out_shape=(
            jax.ShapeDtypeStruct((count, width), bf),
            jax.ShapeDtypeStruct((count, experts), f32),
            jax.ShapeDtypeStruct((count, experts), f32),
        )
        + (jax.ShapeDtypeStruct((slots // n_z, cols), bf),) * n_z,
        in_specs=[in_smem] + [in_vmem] * 3,
        out_specs=(in_vmem,) * (3 + n_z),
        compiler_params=vmem,
        name="pack",
    )(at, tokens, routes, route_weight)
    sent = [along_z(send[z], z, False) for z in range(n_z)]

    gain = lax.dynamic_slice_in_dim(norm_gain, tp_at * cols, cols, 0)
    gate_local = (gate_experts[0] * gain).astype(bf)
    up_local = (up_experts[0] * gain).astype(bf)
    both = jnp.stack([gate_local, up_local], axis=1)
    both = jnp.broadcast_to(both[None], (n_gr, *both.shape)).reshape(n_gr * per_group, 2, rows_here, cols)
    both, sent = lax.optimization_barrier((both, sent))
    both = lax.all_to_all(both, GF, split_axis=0, concat_axis=0, tiled=True)
    down_local = down_experts[0].astype(bf)
    down_all = jnp.broadcast_to(down_local[None], (n_gr, *down_local.shape)).reshape(-1, rows_here, cols)
    down_all = lax.all_to_all(down_all, GF, split_axis=0, concat_axis=0, tiled=True)
    down_w = down_all.reshape(n_gr, n_fs * rows_here, cols)

    reached = []
    for y in range(n_y):
        part = jnp.concatenate([s[y * block_rows : (y + 1) * block_rows] for s in sent], axis=0)
        reached.append(turned_by(part, "y", y))

    sh_rows, sh_cols = gate_shared.shape
    gain_sh = lax.dynamic_slice_in_dim(norm_gain, fs_at * sh_rows, sh_rows, 0)[:, None]
    pair = jnp.concatenate([(gate_shared * gain_sh).astype(bf), (up_shared * gain_sh).astype(bf)], axis=1)
    half = sh_rows * 2 * sh_cols // cols
    times = sh_rows // half
    pair = jnp.concatenate([pair[i * half : (i + 1) * half] for i in range(times)], axis=1)
    block = jnp.concatenate([pair, down_shared.astype(bf)], axis=0)[None]
    block, reached = lax.optimization_barrier((block, reached))
    for axis, n in (("zl", n_z), ("y", n_y)):
        bit = 1
        while bit < n:
            block = jnp.concatenate([block, crossed_with(block, axis, bit)], axis=0)
            bit *= 2

    rows_mine = jnp.concatenate(reached, axis=0)
    rows_mine = [turned_by(rows_mine, "x", n_x - j) for j in range(n_x)]
    rows_other = [crossed_with(r, "core", 1) for r in rows_mine]

    near = n_fs // n_tp
    units = near * rows_here
    both = both.reshape(n_gr, n_x, 2, near, 2, rows_here, cols)
    kept = lax.dynamic_index_in_dim(both, core, 2, keepdims=False)
    given = lax.dynamic_index_in_dim(both, 1 - core, 2, keepdims=False)
    both = jnp.stack([kept, crossed_with(given, "core", 1)], axis=0)

    def for_device(d):
        return lax.dynamic_index_in_dim(both, lax.rem(x_at + d, n_x), 2, keepdims=False)

    pieces = [turned_by(for_device(n_x - j), "x", n_x - j) for j in range(n_x)]

    gate_sw, up_sw, down_sw, shared_hidden = pl.pallas_call(
        functools.partial(shared_kernel, n_z, n_y, half, times),
        out_shape=(
            jax.ShapeDtypeStruct((width, sh_cols), bf),
            jax.ShapeDtypeStruct((width, sh_cols), bf),
            jax.ShapeDtypeStruct((n_fs * down_shared.shape[0], cols), bf),
            jax.ShapeDtypeStruct((sh_cols, count), bf),
        ),
        in_specs=[in_smem, in_vmem, in_vmem],
        out_specs=(in_vmem,) * 4,
        scratch_shapes=[pltpu.VMEM((width, 2 * sh_cols), bf)],
        compiler_params=vmem,
        cost_estimate=pl.CostEstimate(
            flops=4 * count * width * sh_cols, bytes_accessed=4 * width * count, transcendentals=0
        ),
        name="shared",
    )(at, block, normed)

    row_block = slots // 6
    whole = pl.BlockSpec((n_gr, units, width), lambda i: (0, 0, 0))
    hidden, gate_w, up_w = pl.pallas_call(
        functools.partial(hidden_kernel, cap, n_gr),
        out_shape=(
            jax.ShapeDtypeStruct((units, slots + count), bf),
            jax.ShapeDtypeStruct((n_gr, units, width), bf),
            jax.ShapeDtypeStruct((n_gr, units, width), bf),
        ),
        grid=(slots // row_block,),
        in_specs=[in_smem, in_vmem]
        + [pl.BlockSpec((row_block, cols), lambda i: (i, 0))] * n_tp
        + [in_vmem] * n_x,
        out_specs=(pl.BlockSpec((units, slots + count), lambda i: (0, 0)), whole, whole),
        scratch_shapes=[pltpu.VMEM((2 * n_gr * units, width), bf)],
        compiler_params=vmem,
        cost_estimate=pl.CostEstimate(
            flops=4 * n_gr * units * slots * width, bytes_accessed=2 * slots * width, transcendentals=units * slots
        ),
        name="gate_up",
    )(at, shared_hidden, *rows_mine, *rows_other, *pieces)

    mine = [turned_by(hidden, "x", n_x - j) for j in range(n_x)]
    others = [crossed_with(h, "core", 1) for h in mine]
    *picked, shared = pl.pallas_call(
        functools.partial(down_kernel, cap, n_gr, n_y),
        out_shape=(jax.ShapeDtypeStruct((slots // n_y, cols), bf),) * n_y
        + (jax.ShapeDtypeStruct((count, cols), f32),),
        in_specs=[in_smem] + [in_vmem] * (2 + n_tp),
        out_specs=(in_vmem,) * (n_y + 1),
        scratch_shapes=[pltpu.VMEM((n_tp * units, slots + count), bf)],
        compiler_params=vmem,
        cost_estimate=pl.CostEstimate(
            flops=2 * n_gr * slots * n_tp * units * cols, bytes_accessed=2 * slots * n_tp * units, transcendentals=0
        ),
        name="down",
    )(at, down_w, down_sw, *mine, *others)
    picked = [turned_by(picked[y], "y", n_y - y) for y in range(n_y)]
    returned = []
    for z in range(n_z):
        part = jnp.concatenate([p[z * block_rows : (z + 1) * block_rows] for p in picked], axis=0)
        returned.append(along_z(part, z, True))
    mixed = pl.pallas_call(
        functools.partial(mix_kernel, cap, n_z, n_y, experts),
        out_shape=jax.ShapeDtypeStruct((count, cols), bf),
        in_specs=[in_smem] + [in_vmem] * (3 + n_z),
        out_specs=in_vmem,
        compiler_params=vmem,
        name="mix",
    )(at, rank, mix, shared, *returned)
    return (mixed, gate_w[:, None], up_w[:, None], down_w[:, None], gate_sw, up_sw, down_sw)


def solution(mesh):
    gr, fs, tp = mesh.devices.shape
    n_y = 4 if fs % 4 == 0 else 1
    fine = Mesh(mesh.devices.reshape(gr, fs // n_y, n_y, tp // 2, 2), ("gr", "zl", "y", "x", "core"))
    return jax.shard_map(
        on_device,
        mesh=fine,
        in_specs=(
            P(GF, None),
            P(GF, None),
            P(GF, None),
            P(),
            P("gr", None, FS, TP),
            P("gr", None, FS, TP),
            P("gr", None, FS, TP),
            P(FS, TP),
            P(FS, TP),
            P(FS, TP),
        ),
        out_specs=(
            P(GF, TP),
            P(None, FS, TP, None),
            P(None, FS, TP, None),
            P(None, FS, None, TP),
            P(None, TP),
            P(None, TP),
            P(None, TP),
        ),
        check_vma=False,
    )
```

```python
import functools

import jax
import jax.numpy as jnp
from jax import lax
from jax.experimental import pallas as pl
from jax.experimental.pallas import tpu as pltpu
from jax.sharding import Mesh, PartitionSpec as P

EPS = 1e-06
bf = jnp.bfloat16
f32 = jnp.float32
FS = ("zl", "y")
TP = ("x", "core")
GF = ("gr", "zl", "y")


def slot_match(at_ref, rows, experts, cap, n_z, n_y, first, rows_dim):
    shape = (rows, experts) if rows_dim == 0 else (experts, rows)
    r = lax.broadcasted_iota(jnp.int32, shape, rows_dim) + first
    e = lax.broadcasted_iota(jnp.int32, shape, 1 - rows_dim)
    groups = experts // (n_z * n_y)
    k = lax.rem(e, n_z * n_y)
    z_off = lax.rem(lax.div(k, n_y) - at_ref[1] + n_z, n_z)
    y_off = lax.rem(lax.rem(k, n_y) - at_ref[2] + n_y, n_y)
    base = cap * (groups * (z_off * n_y + y_off) + lax.div(e, n_z * n_y))
    inside = (r >= base) & (r < base + cap)
    return jnp.where(inside, 1.0, 0.0).astype(bf)


def slot_number(shape, dim, cap):
    return lax.rem(lax.broadcasted_iota(jnp.int32, shape, dim), cap).astype(f32)


def pack_kernel(at_ref, tok_ref, route_ref, weight_ref, gate_ref, up_ref, gain_ref, down_ref,
                normed_ref, rank_ref, mix_ref, block_ref):
    experts = rank_ref.shape[1]
    cols = block_ref.shape[1]
    values = tok_ref[...].astype(f32)
    scale = lax.rsqrt(jnp.mean(values * values, axis=-1, keepdims=True) + EPS)
    normed_ref[...] = (values * scale).astype(bf)
    count, top = route_ref.shape
    block_ref[:count, :] = normed_ref[:, pl.ds(pl.multiple_of(at_ref[0] * cols, cols), cols)]
    rows, units = gate_ref.shape
    gate = (gate_ref[...] * gain_ref[...]).astype(bf)
    up = (up_ref[...] * gain_ref[...]).astype(bf)
    times = cols // (2 * units)
    half = rows // times
    parts = []
    for i in range(times):
        parts += [gate[i * half : (i + 1) * half], up[i * half : (i + 1) * half]]
    block_ref[count : count + half, :] = jnp.concatenate(parts, axis=1)
    below = count + half + down_ref.shape[0]
    block_ref[count + half : below, :] = down_ref[...].astype(bf)
    lane = lax.broadcasted_iota(jnp.int32, (cols, 128), 1)
    wide = jnp.zeros((cols, 128), f32)
    routes = jnp.concatenate([route_ref[...].astype(f32), jnp.zeros((cols - count, top), f32)], axis=0)
    for j in range(top):
        wide = jnp.where(lane == j, routes[:, j : j + 1], wide)
    block_ref[below:, :] = wide.T[:top].astype(bf)
    e = lax.broadcasted_iota(jnp.int32, (count, experts), 1)
    chosen = jnp.zeros((count, experts), f32)
    mix = jnp.zeros((count, experts), f32)
    for j in range(top):
        here = route_ref[:, j : j + 1] == e
        chosen = jnp.where(here, 1.0, chosen)
        mix = jnp.where(here, weight_ref[:, j : j + 1], mix)
    row = lax.broadcasted_iota(jnp.int32, (count, count), 0)
    col = lax.broadcasted_iota(jnp.int32, (count, count), 1)
    before = jnp.where(col < row, 1.0, 0.0).astype(bf)
    rank = jnp.dot(before, chosen.astype(bf), preferred_element_type=f32)
    rank_ref[...] = jnp.where(chosen > 0, rank, -1.0)
    mix_ref[...] = mix


def select_kernel(cap, n_gr, n_y, count, top, at_ref, *refs):
    n_z = len(refs) - n_y - 1
    blocks, outs, shared_ref = refs[:n_z], refs[n_z:-1], refs[-1]
    here = n_y * n_gr
    rows = here * cap
    row = lax.broadcasted_iota(jnp.int32, (count, count), 0)
    col = lax.broadcasted_iota(jnp.int32, (count, count), 1)
    before = jnp.where(row < col, 1.0, 0.0).astype(bf)
    r = lax.broadcasted_iota(jnp.int32, (here, count), 0)
    y = lax.rem(lax.div(r, n_gr) + at_ref[2], n_y)
    expert = (lax.rem(r, n_gr) * n_z * n_y + at_ref[1] * n_y + y).astype(f32)
    q = lax.broadcasted_iota(jnp.int32, (rows, here), 0)
    first = cap * lax.broadcasted_iota(jnp.int32, (rows, here), 1)
    owner = jnp.where((q >= first) & (q < first + cap), 1.0, 0.0).astype(bf)
    number = slot_number((rows, count), 0, cap)
    each = n_gr * cap
    for i in range(n_z):
        block_ref = blocks[i]
        last = block_ref.shape[0] - top
        routes = block_ref[last:, :count].astype(f32)
        chosen = jnp.zeros((here, count), f32)
        for j in range(top):
            chosen = jnp.where(routes[j : j + 1, :] == expert, 1.0, chosen)
        rank = jnp.dot(chosen.astype(bf), before, preferred_element_type=f32)
        rank = jnp.where(chosen > 0, rank, -1.0).astype(bf)
        pick = jnp.dot(owner, rank, preferred_element_type=f32) == number
        pick = jnp.where(pick, 1.0, 0.0).astype(bf)
        picked = jnp.dot(pick, block_ref[:count, :], preferred_element_type=f32).astype(bf)
        for y_off in range(n_y):
            outs[y_off][i * each : (i + 1) * each, :] = picked[y_off * each : (y_off + 1) * each]
        shared_ref[i] = block_ref[count:last, :]


def shared_kernel(half, times, at_ref, normed_ref, *refs):
    blocks, (gate_ref, up_ref, down_ref, hidden_ref, pair_ref) = refs[:-5], refs[-5:]
    n_y, n_z = len(blocks), blocks[0].shape[0]
    rows = half * times
    both = pair_ref.shape[1]
    below = blocks[0].shape[1] - half
    for j in range(n_y):
        for i in range(n_z):
            p = lax.rem(at_ref[1] - i + n_z, n_z) * n_y + lax.rem(at_ref[2] + j, n_y)
            for t in range(times):
                first = pl.multiple_of(p * rows + t * half, half)
                pair_ref[pl.ds(first, half), :] = blocks[j][i, :half, t * both : (t + 1) * both]
            down_ref[pl.ds(pl.multiple_of(p * below, below), below), :] = blocks[j][i, half:, :]
    pair = pair_ref[...]
    gate_ref[...] = pair[:, : both // 2]
    up_ref[...] = pair[:, both // 2 :]
    turned = jnp.dot(normed_ref[...], pair, preferred_element_type=f32).T
    gate, up = turned[: both // 2], turned[both // 2 :]
    hidden_ref[...] = (gate / (1.0 + jnp.exp(-gate)) * up).astype(bf)


def hidden_kernel(cap, n_gr, at_ref, shared_ref, *refs):
    n_x = (len(refs) - 4) // 3
    rows_refs, pieces, (out_ref, gate_ref, up_ref, w_ref) = refs[: 2 * n_x], refs[2 * n_x : 3 * n_x], refs[3 * n_x :]
    near, rows_here, cols = pieces[0].shape[2], pieces[0].shape[4], pieces[0].shape[5]
    units = near * rows_here
    rows = rows_refs[0].shape[0]

    def lanes_of(c, j):
        core = at_ref[4] if c == 0 else 1 - at_ref[4]
        owner = lax.rem(at_ref[3] + j, n_x) * 2 + core
        return pl.ds(pl.multiple_of(owner * cols, cols), cols)

    @pl.when(pl.program_id(0) == 0)
    def _():
        for j in range(n_x):
            for c in range(2):
                lanes = lanes_of(c, j)
                for g in range(n_gr):
                    for q in range(near):
                        for mat, served in ((0, gate_ref), (1, up_ref)):
                            piece = pieces[j][c, g, q, mat]
                            first = q * rows_here
                            served[g, first : first + rows_here, lanes] = piece
                            first += (2 * g + mat) * units
                            w_ref[first : first + rows_here, lanes] = piece
        out_ref[:, out_ref.shape[1] - shared_ref.shape[1] :] = shared_ref[...]

    total = jnp.zeros((2 * n_gr * units, rows), f32)
    for j in range(n_x):
        for c in range(2):
            w = w_ref[:, lanes_of(c, j)]
            total += lax.dot_general(
                w, rows_refs[c * n_x + j][...], (((1,), (1,)), ((), ())), preferred_element_type=f32
            )
    slot = lax.broadcasted_iota(jnp.int32, (units, rows), 1) + pl.program_id(0) * rows
    group = lax.div(lax.rem(slot, cap * n_gr), cap)
    gate, up = total[:units], total[units : 2 * units]
    for g in range(1, n_gr):
        gate = jnp.where(group == g, total[2 * g * units : (2 * g + 1) * units], gate)
        up = jnp.where(group == g, total[(2 * g + 1) * units : (2 * g + 2) * units], up)
    hidden = (gate / (1.0 + jnp.exp(-gate)) * up).astype(bf)
    out_ref[:, pl.ds(pl.multiple_of(pl.program_id(0) * rows, 128), rows)] = hidden


def down_kernel(cap, n_gr, n_y, at_ref, down_ref, down_sh_ref, *refs):
    pieces, outs, (shared_ref, h_ref) = refs[: -2 - n_y], refs[-2 - n_y : -2], refs[-2:]
    n_x = len(pieces) // 2
    units = pieces[0].shape[0]
    each, cols = outs[0].shape
    for c in range(2):
        core = at_ref[4] if c == 0 else 1 - at_ref[4]
        for j in range(n_x):
            first = (lax.rem(at_ref[3] + j, n_x) * 2 + core) * units
            h_ref[pl.ds(pl.multiple_of(first, units), units), :] = pieces[c * n_x + j][...]
    turn = (((0,), (0,)), ((), ()))
    for pair in range(n_y // 2):
        first = pair * 2 * each
        h = h_ref[:, first : first + 2 * each]
        slot = lax.broadcasted_iota(jnp.int32, (2 * each, cols), 0) + first
        group = lax.div(lax.rem(slot, cap * n_gr), cap)
        picked = lax.dot_general(h, down_ref[0], turn, preferred_element_type=f32)
        for g in range(1, n_gr):
            other = lax.dot_general(h, down_ref[g], turn, preferred_element_type=f32)
            picked = jnp.where(group == g, other, picked)
        picked = picked.astype(bf)
        outs[2 * pair][...] = picked[:each]
        outs[2 * pair + 1][...] = picked[each:]
    slots = n_y * each
    shared_ref[...] = lax.dot_general(h_ref[:, slots:], down_sh_ref[...], turn, preferred_element_type=f32)


def mix_kernel(cap, n_z, n_y, experts, at_ref, rank_ref, mix_ref, shared_ref, *refs):
    parts, out_ref = refs[:-1], refs[-1]
    rank = rank_ref[...].astype(bf)
    high = mix_ref[...].astype(bf)
    low = (mix_ref[...] - high.astype(f32)).astype(bf)
    count = rank.shape[0]
    total = shared_ref[...]
    chunk = parts[0].shape[0]
    number = slot_number((count, chunk), 1, cap)
    for i, part_ref in enumerate(parts):
        owner = slot_match(at_ref, chunk, experts, cap, n_z, n_y, i * chunk, 1)
        pick = jnp.dot(rank, owner, preferred_element_type=f32) == number
        part = part_ref[...]
        for w in (high, low):
            weight = jnp.dot(w, owner, preferred_element_type=f32)
            weight = jnp.where(pick, weight, 0.0).astype(bf)
            total += jnp.dot(weight, part, preferred_element_type=f32)
    out_ref[...] = total.astype(bf)


def turned_by(value, axis, d):
    n = lax.axis_size(axis)
    return lax.ppermute(value, axis, [(i, (i + d) % n) for i in range(n)]) if d % n else value


def crossed_with(value, axis, bit):
    return lax.ppermute(value, axis, [(i, i ^ bit) for i in range(lax.axis_size(axis))])


def over_z(value, shift, back=False):
    n_gr, n_z, n_y = lax.axis_size("gr"), lax.axis_size("zl"), lax.axis_size("y")
    n = n_gr * n_z
    pairs = [(z * n_y + y, (z + shift(y)) % n * n_y + y) for z in range(n) for y in range(n_y)]
    return lax.ppermute(value, GF, [p[::-1] for p in pairs] if back else pairs)


def back_along_z(value, z_off):
    n_z = lax.axis_size("zl")
    if z_off == 0:
        return value
    return over_z(
        value,
        lambda y: z_off if 2 * z_off < n_z or (2 * z_off == n_z and y % 2 == 0) else z_off - n_z,
        True,
    )


def from_all_z(block):
    n_z = lax.axis_size("zl")
    ahead, behind = [block], [block]
    for _ in range(n_z // 2 - 1):
        ahead.append(over_z(ahead[-1], lambda y: 1))
        behind.append(over_z(behind[-1], lambda y: -1))
    even = lax.axis_index("y") % 2 == 0
    far = over_z(jnp.where(even, ahead[-1], behind[-1]), lambda y: 1 if y % 2 == 0 else -1)
    return ahead + [far] + behind[:0:-1]


def from_all_x(value):
    n_x = lax.axis_size("x")
    if n_x != 4:
        return [turned_by(value, "x", n_x - j) for j in range(n_x)]
    half = value.shape[0] // 2
    left, right = turned_by(value, "x", 1), turned_by(value, "x", 3)
    far = [turned_by(left[:half], "x", 1), turned_by(right[half:], "x", 3)]
    return [value, right, jnp.concatenate(far, axis=0), left]


def on_device(tokens, routes, route_weight, norm_gain, gate_experts, up_experts, down_experts,
              gate_shared, up_shared, down_shared):
    n_gr, n_fs, n_tp = lax.axis_size("gr"), lax.axis_size(FS), lax.axis_size(TP)
    n_z, n_y, n_x = lax.axis_size("zl"), lax.axis_size("y"), lax.axis_size("x")
    fs_at, tp_at, x_at, core = lax.axis_index(FS), lax.axis_index(TP), lax.axis_index("x"), lax.axis_index("core")
    at = jnp.stack([tp_at, lax.axis_index("zl"), lax.axis_index("y"), x_at, core]).astype(jnp.int32)
    per_group, rows_here, cols = gate_experts.shape[1:]
    count, top = routes.shape
    width = tokens.shape[1]
    experts = per_group * n_gr
    cap = (3 * count * top + 2 * experts - 1) // (2 * experts)
    slots = experts * cap
    block_rows = n_gr * cap

    in_smem, in_vmem = pl.BlockSpec(memory_space=pltpu.SMEM), pl.BlockSpec(memory_space=pltpu.VMEM)
    vmem = pltpu.CompilerParams(vmem_limit_bytes=48 * 1024 * 1024)
    sh_rows, sh_cols = gate_shared.shape
    half = sh_rows * 2 * sh_cols // cols
    times = sh_rows // half
    gain_sh = lax.dynamic_slice_in_dim(norm_gain, fs_at * sh_rows, sh_rows, 0)[:, None]
    ride = half + down_shared.shape[0]
    normed, rank, mix, block = pl.pallas_call(
        pack_kernel,
        out_shape=(
            jax.ShapeDtypeStruct((count, width), bf),
            jax.ShapeDtypeStruct((count, experts), f32),
            jax.ShapeDtypeStruct((count, experts), f32),
            jax.ShapeDtypeStruct((count + ride + top, cols), bf),
        ),
        in_specs=[in_smem] + [in_vmem] * 7,
        out_specs=(in_vmem,) * 4,
        compiler_params=vmem,
        name="pack",
    )(at, tokens, routes, route_weight, gate_shared, up_shared, gain_sh, down_shared)
    with jax.named_scope("zchain"):
        blocks = from_all_z(block)
    *chosen, ridden = pl.pallas_call(
        functools.partial(select_kernel, cap, n_gr, n_y, count, top),
        out_shape=(jax.ShapeDtypeStruct((slots // n_y, cols), bf),) * n_y
        + (jax.ShapeDtypeStruct((n_z, ride, cols), bf),),
        in_specs=[in_smem] + [in_vmem] * n_z,
        out_specs=(in_vmem,) * (n_y + 1),
        compiler_params=vmem,
        name="select",
    )(at, *blocks)
    with jax.named_scope("yturn"):
        reached = [turned_by(chosen[y], "y", y) for y in range(n_y)]

    gain = lax.dynamic_slice_in_dim(norm_gain, tp_at * cols, cols, 0)
    gate_local = (gate_experts[0] * gain).astype(bf)
    up_local = (up_experts[0] * gain).astype(bf)
    both = jnp.stack([gate_local, up_local], axis=1)
    both = jnp.broadcast_to(both[None], (n_gr, *both.shape)).reshape(n_gr * per_group, 2, rows_here, cols)
    both, ridden, chosen = lax.optimization_barrier((both, ridden, chosen))
    with jax.named_scope("both"):
        both = lax.all_to_all(both, GF, split_axis=0, concat_axis=0, tiled=True)
    down_local = down_experts[0].astype(bf)
    down_all = jnp.broadcast_to(down_local[None], (n_gr, *down_local.shape)).reshape(-1, rows_here, cols)
    down_all = lax.all_to_all(down_all, GF, split_axis=0, concat_axis=0, tiled=True)
    down_w = down_all.reshape(n_gr, n_fs * rows_here, cols)

    rows_mine = from_all_x(jnp.concatenate(reached, axis=0))
    rows_other = [crossed_with(r, "core", 1) for r in rows_mine]
    ridden, reached = lax.optimization_barrier((ridden, reached))
    ridden = [turned_by(ridden, "y", n_y - y) for y in range(n_y)]

    near = n_fs // n_tp
    units = near * rows_here
    both = both.reshape(n_gr, n_x, 2, near, 2, rows_here, cols)
    kept = lax.dynamic_index_in_dim(both, core, 2, keepdims=False)
    given = lax.dynamic_index_in_dim(both, 1 - core, 2, keepdims=False)
    both = jnp.stack([kept, crossed_with(given, "core", 1)], axis=0)

    def for_device(d):
        return lax.dynamic_index_in_dim(both, lax.rem(x_at + d, n_x), 2, keepdims=False)

    pieces = [turned_by(for_device(n_x - j), "x", n_x - j) for j in range(n_x)]

    gate_sw, up_sw, down_sw, shared_hidden = pl.pallas_call(
        functools.partial(shared_kernel, half, times),
        out_shape=(
            jax.ShapeDtypeStruct((width, sh_cols), bf),
            jax.ShapeDtypeStruct((width, sh_cols), bf),
            jax.ShapeDtypeStruct((n_fs * down_shared.shape[0], cols), bf),
            jax.ShapeDtypeStruct((sh_cols, count), bf),
        ),
        in_specs=[in_smem] + [in_vmem] * (1 + n_y),
        out_specs=(in_vmem,) * 4,
        scratch_shapes=[pltpu.VMEM((width, 2 * sh_cols), bf)],
        compiler_params=vmem,
        cost_estimate=pl.CostEstimate(
            flops=4 * count * width * sh_cols, bytes_accessed=4 * width * count, transcendentals=0
        ),
        name="shared",
    )(at, normed, *ridden)

    row_block = slots // 6
    whole = pl.BlockSpec((n_gr, units, width), lambda i: (0, 0, 0))
    hidden, gate_w, up_w = pl.pallas_call(
        functools.partial(hidden_kernel, cap, n_gr),
        out_shape=(
            jax.ShapeDtypeStruct((units, slots + count), bf),
            jax.ShapeDtypeStruct((n_gr, units, width), bf),
            jax.ShapeDtypeStruct((n_gr, units, width), bf),
        ),
        grid=(slots // row_block,),
        in_specs=[in_smem, in_vmem]
        + [pl.BlockSpec((row_block, cols), lambda i: (i, 0))] * n_tp
        + [in_vmem] * n_x,
        out_specs=(pl.BlockSpec((units, slots + count), lambda i: (0, 0)), whole, whole),
        scratch_shapes=[pltpu.VMEM((2 * n_gr * units, width), bf)],
        compiler_params=vmem,
        cost_estimate=pl.CostEstimate(
            flops=4 * n_gr * units * slots * width, bytes_accessed=2 * slots * width, transcendentals=units * slots
        ),
        name="gate_up",
    )(at, shared_hidden, *rows_mine, *rows_other, *pieces)

    mine = [turned_by(hidden, "x", n_x - j) for j in range(n_x)]
    others = [crossed_with(h, "core", 1) for h in mine]
    *picked, shared = pl.pallas_call(
        functools.partial(down_kernel, cap, n_gr, n_y),
        out_shape=(jax.ShapeDtypeStruct((slots // n_y, cols), bf),) * n_y
        + (jax.ShapeDtypeStruct((count, cols), f32),),
        in_specs=[in_smem] + [in_vmem] * (2 + n_tp),
        out_specs=(in_vmem,) * (n_y + 1),
        scratch_shapes=[pltpu.VMEM((n_tp * units, slots + count), bf)],
        compiler_params=vmem,
        cost_estimate=pl.CostEstimate(
            flops=2 * n_gr * slots * n_tp * units * cols, bytes_accessed=2 * slots * n_tp * units, transcendentals=0
        ),
        name="down",
    )(at, down_w, down_sw, *mine, *others)
    picked = [turned_by(picked[y], "y", n_y - y) for y in range(n_y)]
    returned = []
    for z in range(n_z):
        part = jnp.concatenate([p[z * block_rows : (z + 1) * block_rows] for p in picked], axis=0)
        returned.append(back_along_z(part, z))
    mixed = pl.pallas_call(
        functools.partial(mix_kernel, cap, n_z, n_y, experts),
        out_shape=jax.ShapeDtypeStruct((count, cols), bf),
        in_specs=[in_smem] + [in_vmem] * (3 + n_z),
        out_specs=in_vmem,
        compiler_params=vmem,
        name="mix",
    )(at, rank, mix, shared, *returned)
    return (mixed, gate_w[:, None], up_w[:, None], down_w[:, None], gate_sw, up_sw, down_sw)


def solution(mesh):
    gr, fs, tp = mesh.devices.shape
    n_y = 4 if fs % 4 == 0 else 1
    fine = Mesh(mesh.devices.reshape(gr, fs // n_y, n_y, tp // 2, 2), ("gr", "zl", "y", "x", "core"))
    return jax.shard_map(
        on_device,
        mesh=fine,
        in_specs=(
            P(GF, None),
            P(GF, None),
            P(GF, None),
            P(),
            P("gr", None, FS, TP),
            P("gr", None, FS, TP),
            P("gr", None, FS, TP),
            P(FS, TP),
            P(FS, TP),
            P(FS, TP),
        ),
        out_specs=(
            P(GF, TP),
            P(None, FS, TP, None),
            P(None, FS, TP, None),
            P(None, FS, None, TP),
            P(None, TP),
            P(None, TP),
            P(None, TP),
        ),
        check_vma=False,
    )
```

```python
import functools

import jax
import jax.numpy as jnp
from jax import lax
from jax.experimental import pallas as pl
from jax.experimental.pallas import tpu as pltpu
from jax.sharding import Mesh, PartitionSpec as P

EPS = 1e-06
bf = jnp.bfloat16
f32 = jnp.float32
FS = ("zl", "y")
TP = ("x", "core")
GF = ("gr", "zl", "y")


def slot_match(at_ref, rows, experts, cap, n_z, n_y, first, rows_dim):
    shape = (rows, experts) if rows_dim == 0 else (experts, rows)
    r = lax.broadcasted_iota(jnp.int32, shape, rows_dim) + first
    e = lax.broadcasted_iota(jnp.int32, shape, 1 - rows_dim)
    groups = experts // (n_z * n_y)
    k = lax.rem(e, n_z * n_y)
    z_off = lax.rem(lax.div(k, n_y) - at_ref[1] + n_z, n_z)
    y_off = lax.rem(lax.rem(k, n_y) - at_ref[2] + n_y, n_y)
    base = cap * (groups * (y_off * n_z + z_off) + lax.div(e, n_z * n_y))
    inside = (r >= base) & (r < base + cap)
    return jnp.where(inside, 1.0, 0.0).astype(bf)


def slot_number(shape, dim, cap):
    return lax.rem(lax.broadcasted_iota(jnp.int32, shape, dim), cap).astype(f32)


def pack_kernel(at_ref, tok_ref, route_ref, weight_ref, gate_ref, up_ref, gain_ref, down_ref,
                normed_ref, rank_ref, mix_ref, block_ref):
    experts = rank_ref.shape[1]
    cols = block_ref.shape[1]
    values = tok_ref[...].astype(f32)
    scale = lax.rsqrt(jnp.mean(values * values, axis=-1, keepdims=True) + EPS)
    normed_ref[...] = (values * scale).astype(bf)
    count, top = route_ref.shape
    block_ref[:count, :] = normed_ref[:, pl.ds(pl.multiple_of(at_ref[0] * cols, cols), cols)]
    rows, units = gate_ref.shape
    gate = (gate_ref[...] * gain_ref[...]).astype(bf)
    up = (up_ref[...] * gain_ref[...]).astype(bf)
    times = cols // (2 * units)
    half = rows // times
    parts = []
    for i in range(times):
        parts += [gate[i * half : (i + 1) * half], up[i * half : (i + 1) * half]]
    block_ref[count : count + half, :] = jnp.concatenate(parts, axis=1)
    below = count + half + down_ref.shape[0]
    block_ref[count + half : below, :] = down_ref[...].astype(bf)
    lane = lax.broadcasted_iota(jnp.int32, (cols, 128), 1)
    wide = jnp.zeros((cols, 128), f32)
    routes = jnp.concatenate([route_ref[...].astype(f32), jnp.zeros((cols - count, top), f32)], axis=0)
    for j in range(top):
        wide = jnp.where(lane == j, routes[:, j : j + 1], wide)
    block_ref[below:, :] = wide.T[:top].astype(bf)
    e = lax.broadcasted_iota(jnp.int32, (count, experts), 1)
    chosen = jnp.zeros((count, experts), f32)
    mix = jnp.zeros((count, experts), f32)
    for j in range(top):
        here = route_ref[:, j : j + 1] == e
        chosen = jnp.where(here, 1.0, chosen)
        mix = jnp.where(here, weight_ref[:, j : j + 1], mix)
    row = lax.broadcasted_iota(jnp.int32, (count, count), 0)
    col = lax.broadcasted_iota(jnp.int32, (count, count), 1)
    before = jnp.where(col < row, 1.0, 0.0).astype(bf)
    rank = jnp.dot(before, chosen.astype(bf), preferred_element_type=f32)
    rank_ref[...] = jnp.where(chosen > 0, rank, -1.0)
    mix_ref[...] = mix


def select_kernel(cap, n_gr, n_y, count, top, at_ref, *refs):
    n_z = len(refs) - n_y - 1
    blocks, outs, shared_ref = refs[:n_z], refs[n_z:-1], refs[-1]
    here = n_y * n_gr
    rows = here * cap
    row = lax.broadcasted_iota(jnp.int32, (count, count), 0)
    col = lax.broadcasted_iota(jnp.int32, (count, count), 1)
    before = jnp.where(row < col, 1.0, 0.0).astype(bf)
    r = lax.broadcasted_iota(jnp.int32, (here, count), 0)
    y = lax.rem(lax.div(r, n_gr) + at_ref[2], n_y)
    expert = (lax.rem(r, n_gr) * n_z * n_y + at_ref[1] * n_y + y).astype(f32)
    q = lax.broadcasted_iota(jnp.int32, (rows, here), 0)
    first = cap * lax.broadcasted_iota(jnp.int32, (rows, here), 1)
    owner = jnp.where((q >= first) & (q < first + cap), 1.0, 0.0).astype(bf)
    number = slot_number((rows, count), 0, cap)
    each = n_gr * cap
    for i in range(n_z):
        block_ref = blocks[i]
        last = block_ref.shape[0] - top
        routes = block_ref[last:, :count].astype(f32)
        chosen = jnp.zeros((here, count), f32)
        for j in range(top):
            chosen = jnp.where(routes[j : j + 1, :] == expert, 1.0, chosen)
        rank = jnp.dot(chosen.astype(bf), before, preferred_element_type=f32)
        rank = jnp.where(chosen > 0, rank, -1.0).astype(bf)
        pick = jnp.dot(owner, rank, preferred_element_type=f32) == number
        pick = jnp.where(pick, 1.0, 0.0).astype(bf)
        picked = jnp.dot(pick, block_ref[:count, :], preferred_element_type=f32).astype(bf)
        for y_off in range(n_y):
            outs[y_off][i * each : (i + 1) * each, :] = picked[y_off * each : (y_off + 1) * each]
        shared_ref[i] = block_ref[count:last, :]


def shared_kernel(half, times, at_ref, normed_ref, *refs):
    blocks, (gate_ref, up_ref, down_ref, hidden_ref, pair_ref) = refs[:-5], refs[-5:]
    n_y, n_z = len(blocks), blocks[0].shape[0]
    rows = half * times
    both = pair_ref.shape[1]
    below = blocks[0].shape[1] - half
    for j in range(n_y):
        for i in range(n_z):
            p = lax.rem(at_ref[1] - i + n_z, n_z) * n_y + lax.rem(at_ref[2] + j, n_y)
            for t in range(times):
                first = pl.multiple_of(p * rows + t * half, half)
                pair_ref[pl.ds(first, half), :] = blocks[j][i, :half, t * both : (t + 1) * both]
            down_ref[pl.ds(pl.multiple_of(p * below, below), below), :] = blocks[j][i, half:, :]
    pair = pair_ref[...]
    gate_ref[...] = pair[:, : both // 2]
    up_ref[...] = pair[:, both // 2 :]
    turned = jnp.dot(normed_ref[...], pair, preferred_element_type=f32).T
    gate, up = turned[: both // 2], turned[both // 2 :]
    hidden_ref[...] = (gate / (1.0 + jnp.exp(-gate)) * up).astype(bf)


def hidden_kernel(cap, n_gr, at_ref, shared_ref, *refs):
    n_x = (len(refs) - 4) // 3
    rows_refs, pieces, (out_ref, gate_ref, up_ref, w_ref) = refs[: 2 * n_x], refs[2 * n_x : 3 * n_x], refs[3 * n_x :]
    near, rows_here, cols = pieces[0].shape[2], pieces[0].shape[4], pieces[0].shape[5]
    units = near * rows_here
    rows = rows_refs[0].shape[0]

    def lanes_of(c, j):
        core = at_ref[4] if c == 0 else 1 - at_ref[4]
        owner = lax.rem(at_ref[3] + j, n_x) * 2 + core
        return pl.ds(pl.multiple_of(owner * cols, cols), cols)

    @pl.when(pl.program_id(0) == 0)
    def _():
        for j in range(n_x):
            for c in range(2):
                lanes = lanes_of(c, j)
                for g in range(n_gr):
                    for q in range(near):
                        for mat, served in ((0, gate_ref), (1, up_ref)):
                            piece = pieces[j][c, g, q, mat]
                            first = q * rows_here
                            served[g, first : first + rows_here, lanes] = piece
                            first += (2 * g + mat) * units
                            w_ref[first : first + rows_here, lanes] = piece
        out_ref[:, out_ref.shape[1] - shared_ref.shape[1] :] = shared_ref[...]

    total = jnp.zeros((2 * n_gr * units, rows), f32)
    for j in range(n_x):
        for c in range(2):
            w = w_ref[:, lanes_of(c, j)]
            total += lax.dot_general(
                w, rows_refs[c * n_x + j][...], (((1,), (1,)), ((), ())), preferred_element_type=f32
            )
    slot = lax.broadcasted_iota(jnp.int32, (units, rows), 1) + pl.program_id(0) * rows
    group = lax.div(lax.rem(slot, cap * n_gr), cap)
    gate, up = total[:units], total[units : 2 * units]
    for g in range(1, n_gr):
        gate = jnp.where(group == g, total[2 * g * units : (2 * g + 1) * units], gate)
        up = jnp.where(group == g, total[(2 * g + 1) * units : (2 * g + 2) * units], up)
    hidden = (gate / (1.0 + jnp.exp(-gate)) * up).astype(bf)
    out_ref[:, pl.ds(pl.multiple_of(pl.program_id(0) * rows, 128), rows)] = hidden


def down_kernel(cap, n_gr, n_y, n_z, at_ref, down_ref, down_sh_ref, *refs):
    pieces, outs, (shared_ref, h_ref) = refs[: -2 - n_z], refs[-2 - n_z : -2], refs[-2:]
    n_x = len(pieces) // 2
    units = pieces[0].shape[0]
    cols = shared_ref.shape[1]
    each = n_gr * cap
    for c in range(2):
        core = at_ref[4] if c == 0 else 1 - at_ref[4]
        for j in range(n_x):
            first = (lax.rem(at_ref[3] + j, n_x) * 2 + core) * units
            h_ref[pl.ds(pl.multiple_of(first, units), units), :] = pieces[c * n_x + j][...]
    turn = (((0,), (0,)), ((), ()))
    chunk = 2 * n_z * each
    for pair in range(n_y // 2):
        first = pair * chunk
        h = h_ref[:, first : first + chunk]
        slot = lax.broadcasted_iota(jnp.int32, (chunk, cols), 0) + first
        group = lax.div(lax.rem(slot, cap * n_gr), cap)
        picked = lax.dot_general(h, down_ref[0], turn, preferred_element_type=f32)
        for g in range(1, n_gr):
            other = lax.dot_general(h, down_ref[g], turn, preferred_element_type=f32)
            picked = jnp.where(group == g, other, picked)
        picked = picked.astype(bf)
        for a in range(2):
            y_off = 2 * pair + a
            for z_off in range(n_z):
                start = (a * n_z + z_off) * each
                at = (y_off // 2 + y_off % 2 * (n_y // 2)) * each
                outs[z_off][at : at + each, :] = picked[start : start + each]
    slots = n_y * n_z * each
    shared_ref[...] = lax.dot_general(h_ref[:, slots:], down_sh_ref[...], turn, preferred_element_type=f32)


def mix_kernel(cap, n_z, n_y, experts, at_ref, rank_ref, mix_ref, shared_ref, *refs):
    parts, out_ref = refs[:-1], refs[-1]
    rank = rank_ref[...].astype(bf)
    high = mix_ref[...].astype(bf)
    low = (mix_ref[...] - high.astype(f32)).astype(bf)
    count = rank.shape[0]
    total = shared_ref[...]
    chunk = parts[0].shape[0]
    number = slot_number((count, chunk), 1, cap)
    for i, part_ref in enumerate(parts):
        owner = slot_match(at_ref, chunk, experts, cap, n_z, n_y, i * chunk, 1)
        pick = jnp.dot(rank, owner, preferred_element_type=f32) == number
        part = part_ref[...]
        for w in (high, low):
            weight = jnp.dot(w, owner, preferred_element_type=f32)
            weight = jnp.where(pick, weight, 0.0).astype(bf)
            total += jnp.dot(weight, part, preferred_element_type=f32)
    out_ref[...] = total.astype(bf)


def turned_by(value, axis, d):
    n = lax.axis_size(axis)
    return lax.ppermute(value, axis, [(i, (i + d) % n) for i in range(n)]) if d % n else value


def crossed_with(value, axis, bit):
    return lax.ppermute(value, axis, [(i, i ^ bit) for i in range(lax.axis_size(axis))])


def over_z(value, shift, back=False):
    n_gr, n_z, n_y = lax.axis_size("gr"), lax.axis_size("zl"), lax.axis_size("y")
    n = n_gr * n_z
    pairs = [(z * n_y + y, (z + shift(y)) % n * n_y + y) for z in range(n) for y in range(n_y)]
    return lax.ppermute(value, GF, [p[::-1] for p in pairs] if back else pairs)


def back_along_z(value, z_off):
    n_z = lax.axis_size("zl")
    if z_off == 0:
        return value
    if 2 * z_off != n_z:
        return over_z(value, lambda y: z_off if 2 * z_off < n_z else z_off - n_z, True)
    half = value.shape[0] // 2
    same = over_z(value[:half], lambda y: -z_off if y % 2 else z_off, True)
    other = over_z(value[half:], lambda y: z_off if y % 2 else -z_off, True)
    return jnp.concatenate([same, other], axis=0)


def from_all_z(block, weights):
    n_z = lax.axis_size("zl")
    ahead, behind = [block], [block]
    for _ in range(n_z // 2 - 1):
        ahead.append(over_z(ahead[-1], lambda y: 1))
        behind.append(over_z(behind[-1], lambda y: -1))
    ahead, behind, weights = lax.optimization_barrier((ahead, behind, weights))
    even = lax.axis_index("y") % 2 == 0
    far = over_z(jnp.where(even, ahead[-1], behind[-1]), lambda y: 1 if y % 2 == 0 else -1)
    return ahead + [far] + behind[:0:-1], weights


def from_all_x(value, beside=()):
    n_x = lax.axis_size("x")
    if n_x != 4:
        return [turned_by(value, "x", n_x - j) for j in range(n_x)], beside
    half = value.shape[0] // 2
    left, right = turned_by(value, "x", 1), turned_by(value, "x", 3)
    left, right, beside = lax.optimization_barrier((left, right, beside))
    far = [turned_by(left[:half], "x", 1), turned_by(right[half:], "x", 3)]
    return [value, right, jnp.concatenate(far, axis=0), left], beside


def on_device(tokens, routes, route_weight, norm_gain, gate_experts, up_experts, down_experts,
              gate_shared, up_shared, down_shared):
    n_gr, n_fs, n_tp = lax.axis_size("gr"), lax.axis_size(FS), lax.axis_size(TP)
    n_z, n_y, n_x = lax.axis_size("zl"), lax.axis_size("y"), lax.axis_size("x")
    fs_at, tp_at, x_at, core = lax.axis_index(FS), lax.axis_index(TP), lax.axis_index("x"), lax.axis_index("core")
    at = jnp.stack([tp_at, lax.axis_index("zl"), lax.axis_index("y"), x_at, core]).astype(jnp.int32)
    per_group, rows_here, cols = gate_experts.shape[1:]
    count, top = routes.shape
    width = tokens.shape[1]
    experts = per_group * n_gr
    cap = (3 * count * top + 2 * experts - 1) // (2 * experts)
    slots = experts * cap
    block_rows = n_gr * cap

    in_smem, in_vmem = pl.BlockSpec(memory_space=pltpu.SMEM), pl.BlockSpec(memory_space=pltpu.VMEM)
    vmem = pltpu.CompilerParams(vmem_limit_bytes=48 * 1024 * 1024)
    sh_rows, sh_cols = gate_shared.shape
    half = sh_rows * 2 * sh_cols // cols
    times = sh_rows // half
    gain_sh = lax.dynamic_slice_in_dim(norm_gain, fs_at * sh_rows, sh_rows, 0)[:, None]
    ride = half + down_shared.shape[0]
    normed, rank, mix, block = pl.pallas_call(
        pack_kernel,
        out_shape=(
            jax.ShapeDtypeStruct((count, width), bf),
            jax.ShapeDtypeStruct((count, experts), f32),
            jax.ShapeDtypeStruct((count, experts), f32),
            jax.ShapeDtypeStruct((count + ride + top, cols), bf),
        ),
        in_specs=[in_smem] + [in_vmem] * 7,
        out_specs=(in_vmem,) * 4,
        compiler_params=vmem,
        name="pack",
    )(at, tokens, routes, route_weight, gate_shared, up_shared, gain_sh, down_shared)
    gain = lax.dynamic_slice_in_dim(norm_gain, tp_at * cols, cols, 0)
    weights = [(gate_experts[0] * gain).astype(bf), (up_experts[0] * gain).astype(bf), down_experts[0].astype(bf)]
    weights = jnp.stack(weights, axis=1)
    weights = jnp.broadcast_to(weights[None], (n_gr, *weights.shape)).reshape(-1, 3, rows_here, cols)
    with jax.named_scope("zchain"):
        blocks, weights = from_all_z(block, weights)
    *chosen, ridden = pl.pallas_call(
        functools.partial(select_kernel, cap, n_gr, n_y, count, top),
        out_shape=(jax.ShapeDtypeStruct((slots // n_y, cols), bf),) * n_y
        + (jax.ShapeDtypeStruct((n_z, ride, cols), bf),),
        in_specs=[in_smem] + [in_vmem] * n_z,
        out_specs=(in_vmem,) * (n_y + 1),
        compiler_params=vmem,
        name="select",
    )(at, *blocks)
    with jax.named_scope("yturn"):
        reached = [turned_by(chosen[y], "y", y) for y in range(n_y)]

    with jax.named_scope("weights"):
        weights = lax.all_to_all(weights, GF, split_axis=0, concat_axis=0, tiled=True)
    down_w = weights[:, 2].reshape(n_gr, n_fs * rows_here, cols)

    ridden, reached = lax.optimization_barrier((ridden, reached))
    ridden = [turned_by(ridden, "y", n_y - y) for y in range(n_y)]
    rows_mine, ridden = from_all_x(jnp.concatenate(reached, axis=0), ridden)
    rows_other = [crossed_with(r, "core", 1) for r in rows_mine]

    near = n_fs // n_tp
    units = near * rows_here
    both = weights.reshape(n_gr, n_x, 2, near, 3, rows_here, cols)[:, :, :, :, :2]
    kept = lax.dynamic_index_in_dim(both, core, 2, keepdims=False)
    given = lax.dynamic_index_in_dim(both, 1 - core, 2, keepdims=False)
    both = jnp.stack([kept, crossed_with(given, "core", 1)], axis=0)

    def for_device(d):
        return lax.dynamic_index_in_dim(both, lax.rem(x_at + d, n_x), 2, keepdims=False)

    pieces = [turned_by(for_device(n_x - j), "x", n_x - j) for j in range(n_x)]

    gate_sw, up_sw, down_sw, shared_hidden = pl.pallas_call(
        functools.partial(shared_kernel, half, times),
        out_shape=(
            jax.ShapeDtypeStruct((width, sh_cols), bf),
            jax.ShapeDtypeStruct((width, sh_cols), bf),
            jax.ShapeDtypeStruct((n_fs * down_shared.shape[0], cols), bf),
            jax.ShapeDtypeStruct((sh_cols, count), bf),
        ),
        in_specs=[in_smem] + [in_vmem] * (1 + n_y),
        out_specs=(in_vmem,) * 4,
        scratch_shapes=[pltpu.VMEM((width, 2 * sh_cols), bf)],
        compiler_params=vmem,
        cost_estimate=pl.CostEstimate(
            flops=4 * count * width * sh_cols, bytes_accessed=4 * width * count, transcendentals=0
        ),
        name="shared",
    )(at, normed, *ridden)

    row_block = slots // 6
    whole = pl.BlockSpec((n_gr, units, width), lambda i: (0, 0, 0))
    hidden, gate_w, up_w = pl.pallas_call(
        functools.partial(hidden_kernel, cap, n_gr),
        out_shape=(
            jax.ShapeDtypeStruct((units, slots + count), bf),
            jax.ShapeDtypeStruct((n_gr, units, width), bf),
            jax.ShapeDtypeStruct((n_gr, units, width), bf),
        ),
        grid=(slots // row_block,),
        in_specs=[in_smem, in_vmem]
        + [pl.BlockSpec((row_block, cols), lambda i: (i, 0))] * n_tp
        + [in_vmem] * n_x,
        out_specs=(pl.BlockSpec((units, slots + count), lambda i: (0, 0)), whole, whole),
        scratch_shapes=[pltpu.VMEM((2 * n_gr * units, width), bf)],
        compiler_params=vmem,
        cost_estimate=pl.CostEstimate(
            flops=4 * n_gr * units * slots * width, bytes_accessed=2 * slots * width, transcendentals=units * slots
        ),
        name="gate_up",
    )(at, shared_hidden, *rows_mine, *rows_other, *pieces)

    mine, _ = from_all_x(hidden)
    others = [crossed_with(h, "core", 1) for h in mine]
    *picked, shared = pl.pallas_call(
        functools.partial(down_kernel, cap, n_gr, n_y, n_z),
        out_shape=(jax.ShapeDtypeStruct((slots // n_z, cols), bf),) * n_z
        + (jax.ShapeDtypeStruct((count, cols), f32),),
        in_specs=[in_smem] + [in_vmem] * (2 + n_tp),
        out_specs=(in_vmem,) * (n_z + 1),
        scratch_shapes=[pltpu.VMEM((n_tp * units, slots + count), bf)],
        compiler_params=vmem,
        cost_estimate=pl.CostEstimate(
            flops=2 * n_gr * slots * n_tp * units * cols, bytes_accessed=2 * slots * n_tp * units, transcendentals=0
        ),
        name="down",
    )(at, down_w, down_sw, *mine, *others)
    picked = [back_along_z(picked[z], z) for z in range(n_z)]
    returned = []
    for y in range(n_y):
        first = (y // 2 + y % 2 * (n_y // 2)) * block_rows
        part = jnp.concatenate([p[first : first + block_rows] for p in picked], axis=0)
        returned.append(turned_by(part, "y", n_y - y))
    mixed = pl.pallas_call(
        functools.partial(mix_kernel, cap, n_z, n_y, experts),
        out_shape=jax.ShapeDtypeStruct((count, cols), bf),
        in_specs=[in_smem] + [in_vmem] * (3 + n_y),
        out_specs=in_vmem,
        compiler_params=vmem,
        name="mix",
    )(at, rank, mix, shared, *returned)
    return (mixed, gate_w[:, None], up_w[:, None], down_w[:, None], gate_sw, up_sw, down_sw)


def solution(mesh):
    gr, fs, tp = mesh.devices.shape
    n_y = 4 if fs % 4 == 0 else 1
    fine = Mesh(mesh.devices.reshape(gr, fs // n_y, n_y, tp // 2, 2), ("gr", "zl", "y", "x", "core"))
    return jax.shard_map(
        on_device,
        mesh=fine,
        in_specs=(
            P(GF, None),
            P(GF, None),
            P(GF, None),
            P(),
            P("gr", None, FS, TP),
            P("gr", None, FS, TP),
            P("gr", None, FS, TP),
            P(FS, TP),
            P(FS, TP),
            P(FS, TP),
        ),
        out_specs=(
            P(GF, TP),
            P(None, FS, TP, None),
            P(None, FS, TP, None),
            P(None, FS, None, TP),
            P(None, TP),
            P(None, TP),
            P(None, TP),
        ),
        check_vma=False,
    )
```

```python
import functools

import jax
import jax.numpy as jnp
from jax import lax
from jax.experimental import pallas as pl
from jax.experimental.pallas import tpu as pltpu
from jax.sharding import Mesh, PartitionSpec as P

EPS = 1e-06
bf = jnp.bfloat16
f32 = jnp.float32
FS = ("zl", "y")
TP = ("x", "core")
GF = ("gr", "zl", "y")


def slot_match(at_ref, rows, experts, cap, n_z, n_y, first, rows_dim):
    shape = (rows, experts) if rows_dim == 0 else (experts, rows)
    r = lax.broadcasted_iota(jnp.int32, shape, rows_dim) + first
    e = lax.broadcasted_iota(jnp.int32, shape, 1 - rows_dim)
    groups = experts // (n_z * n_y)
    k = lax.rem(e, n_z * n_y)
    z_off = lax.rem(lax.div(k, n_y) - at_ref[1] + n_z, n_z)
    y_off = lax.rem(lax.rem(k, n_y) - at_ref[2] + n_y, n_y)
    base = cap * (groups * (z_off * n_y + y_off) + lax.div(e, n_z * n_y))
    inside = (r >= base) & (r < base + cap)
    return jnp.where(inside, 1.0, 0.0).astype(bf)


def slot_number(shape, dim, cap):
    return lax.rem(lax.broadcasted_iota(jnp.int32, shape, dim), cap).astype(f32)


def pack_kernel(at_ref, tok_ref, route_ref, weight_ref, gate_ref, up_ref, gain_ref, down_ref,
                normed_ref, rank_ref, mix_ref, block_ref):
    experts = rank_ref.shape[1]
    cols = block_ref.shape[1]
    values = tok_ref[...].astype(f32)
    scale = lax.rsqrt(jnp.mean(values * values, axis=-1, keepdims=True) + EPS)
    normed_ref[...] = (values * scale).astype(bf)
    count, top = route_ref.shape
    block_ref[:count, :] = normed_ref[:, pl.ds(pl.multiple_of(at_ref[0] * cols, cols), cols)]
    rows, units = gate_ref.shape
    gate = (gate_ref[...] * gain_ref[...]).astype(bf)
    up = (up_ref[...] * gain_ref[...]).astype(bf)
    times = cols // (2 * units)
    half = rows // times
    parts = []
    for i in range(times):
        parts += [gate[i * half : (i + 1) * half], up[i * half : (i + 1) * half]]
    block_ref[count : count + half, :] = jnp.concatenate(parts, axis=1)
    below = count + half + down_ref.shape[0]
    block_ref[count + half : below, :] = down_ref[...].astype(bf)
    lane = lax.broadcasted_iota(jnp.int32, (cols, 128), 1)
    wide = jnp.zeros((cols, 128), f32)
    routes = jnp.concatenate([route_ref[...].astype(f32), jnp.zeros((cols - count, top), f32)], axis=0)
    for j in range(top):
        wide = jnp.where(lane == j, routes[:, j : j + 1], wide)
    block_ref[below:, :] = wide.T[:top].astype(bf)
    e = lax.broadcasted_iota(jnp.int32, (count, experts), 1)
    chosen = jnp.zeros((count, experts), f32)
    mix = jnp.zeros((count, experts), f32)
    for j in range(top):
        here = route_ref[:, j : j + 1] == e
        chosen = jnp.where(here, 1.0, chosen)
        mix = jnp.where(here, weight_ref[:, j : j + 1], mix)
    row = lax.broadcasted_iota(jnp.int32, (count, count), 0)
    col = lax.broadcasted_iota(jnp.int32, (count, count), 1)
    before = jnp.where(col < row, 1.0, 0.0).astype(bf)
    rank = jnp.dot(before, chosen.astype(bf), preferred_element_type=f32)
    rank_ref[...] = jnp.where(chosen > 0, rank, -1.0)
    mix_ref[...] = mix


def select_kernel(cap, n_gr, n_y, count, top, at_ref, *refs):
    n_z = len(refs) - n_y - 1
    blocks, outs, shared_ref = refs[:n_z], refs[n_z:-1], refs[-1]
    here = n_y * n_gr
    rows = here * cap
    row = lax.broadcasted_iota(jnp.int32, (count, count), 0)
    col = lax.broadcasted_iota(jnp.int32, (count, count), 1)
    before = jnp.where(row < col, 1.0, 0.0).astype(bf)
    r = lax.broadcasted_iota(jnp.int32, (here, count), 0)
    y = lax.rem(lax.div(r, n_gr) + at_ref[2], n_y)
    expert = (lax.rem(r, n_gr) * n_z * n_y + at_ref[1] * n_y + y).astype(f32)
    q = lax.broadcasted_iota(jnp.int32, (rows, here), 0)
    first = cap * lax.broadcasted_iota(jnp.int32, (rows, here), 1)
    owner = jnp.where((q >= first) & (q < first + cap), 1.0, 0.0).astype(bf)
    number = slot_number((rows, count), 0, cap)
    each = n_gr * cap
    for i in range(n_z):
        block_ref = blocks[i]
        last = block_ref.shape[0] - top
        routes = block_ref[last:, :count].astype(f32)
        chosen = jnp.zeros((here, count), f32)
        for j in range(top):
            chosen = jnp.where(routes[j : j + 1, :] == expert, 1.0, chosen)
        rank = jnp.dot(chosen.astype(bf), before, preferred_element_type=f32)
        rank = jnp.where(chosen > 0, rank, -1.0).astype(bf)
        pick = jnp.dot(owner, rank, preferred_element_type=f32) == number
        pick = jnp.where(pick, 1.0, 0.0).astype(bf)
        picked = jnp.dot(pick, block_ref[:count, :], preferred_element_type=f32).astype(bf)
        for y_off in range(n_y):
            outs[y_off][i * each : (i + 1) * each, :] = picked[y_off * each : (y_off + 1) * each]
        shared_ref[i] = block_ref[count:last, :]


def shared_kernel(half, times, at_ref, normed_ref, *refs):
    blocks, (gate_ref, up_ref, down_ref, hidden_ref, pair_ref) = refs[:-5], refs[-5:]
    n_y, n_z = len(blocks), blocks[0].shape[0]
    rows = half * times
    both = pair_ref.shape[1]
    below = blocks[0].shape[1] - half
    for j in range(n_y):
        for i in range(n_z):
            p = lax.rem(at_ref[1] - i + n_z, n_z) * n_y + lax.rem(at_ref[2] + j, n_y)
            for t in range(times):
                first = pl.multiple_of(p * rows + t * half, half)
                pair_ref[pl.ds(first, half), :] = blocks[j][i, :half, t * both : (t + 1) * both]
            down_ref[pl.ds(pl.multiple_of(p * below, below), below), :] = blocks[j][i, half:, :]
    pair = pair_ref[...]
    gate_ref[...] = pair[:, : both // 2]
    up_ref[...] = pair[:, both // 2 :]
    turned = jnp.dot(normed_ref[...], pair, preferred_element_type=f32).T
    gate, up = turned[: both // 2], turned[both // 2 :]
    hidden_ref[...] = (gate / (1.0 + jnp.exp(-gate)) * up).astype(bf)


def hidden_kernel(cap, n_gr, at_ref, shared_ref, both_ref, *refs):
    rows_refs, (out_ref, gate_ref, up_ref, w_ref) = refs[:-4], refs[-4:]
    n_x = len(rows_refs) // 2
    near, rows_here, cols = both_ref.shape[2], both_ref.shape[4], both_ref.shape[5]
    units = near * rows_here
    rows = rows_refs[0].shape[0]

    def lanes_of(c, j):
        core = at_ref[4] if c == 0 else 1 - at_ref[4]
        owner = lax.rem(at_ref[3] + j, n_x) * 2 + core
        return pl.ds(pl.multiple_of(owner * cols, cols), cols)

    @pl.when(pl.program_id(0) == 0)
    def _():
        for p in range(2 * n_x):
            lanes = slice(p * cols, (p + 1) * cols)
            for g in range(n_gr):
                for q in range(near):
                    for mat, served in ((0, gate_ref), (1, up_ref)):
                        piece = both_ref[p, g, q, mat]
                        first = q * rows_here
                        served[g, first : first + rows_here, lanes] = piece
                        first += (2 * g + mat) * units
                        w_ref[first : first + rows_here, lanes] = piece
        out_ref[:, out_ref.shape[1] - shared_ref.shape[1] :] = shared_ref[...]

    total = jnp.zeros((2 * n_gr * units, rows), f32)
    for j in range(n_x):
        for c in range(2):
            w = w_ref[:, lanes_of(c, j)]
            total += lax.dot_general(
                w, rows_refs[c * n_x + j][...], (((1,), (1,)), ((), ())), preferred_element_type=f32
            )
    slot = lax.broadcasted_iota(jnp.int32, (units, rows), 1) + pl.program_id(0) * rows
    group = lax.div(lax.rem(slot, cap * n_gr), cap)
    gate, up = total[:units], total[units : 2 * units]
    for g in range(1, n_gr):
        gate = jnp.where(group == g, total[2 * g * units : (2 * g + 1) * units], gate)
        up = jnp.where(group == g, total[(2 * g + 1) * units : (2 * g + 2) * units], up)
    hidden = (gate / (1.0 + jnp.exp(-gate)) * up).astype(bf)
    out_ref[:, pl.ds(pl.multiple_of(pl.program_id(0) * rows, 128), rows)] = hidden


def down_kernel(cap, n_gr, n_y, at_ref, down_ref, down_sh_ref, *refs):
    pieces, outs, (shared_ref, h_ref) = refs[: -2 - n_y], refs[-2 - n_y : -2], refs[-2:]
    n_x = len(pieces) // 2
    units = pieces[0].shape[0]
    each, cols = outs[0].shape
    for c in range(2):
        core = at_ref[4] if c == 0 else 1 - at_ref[4]
        for j in range(n_x):
            first = (lax.rem(at_ref[3] + j, n_x) * 2 + core) * units
            h_ref[pl.ds(pl.multiple_of(first, units), units), :] = pieces[c * n_x + j][...]
    turn = (((0,), (0,)), ((), ()))
    for pair in range(n_y // 2):
        first = pair * 2 * each
        h = h_ref[:, first : first + 2 * each]
        slot = lax.broadcasted_iota(jnp.int32, (2 * each, cols), 0) + first
        group = lax.div(lax.rem(slot, cap * n_gr), cap)
        picked = lax.dot_general(h, down_ref[0], turn, preferred_element_type=f32)
        for g in range(1, n_gr):
            other = lax.dot_general(h, down_ref[g], turn, preferred_element_type=f32)
            picked = jnp.where(group == g, other, picked)
        picked = picked.astype(bf)
        outs[2 * pair][...] = picked[:each]
        outs[2 * pair + 1][...] = picked[each:]
    slots = n_y * each
    shared_ref[...] = lax.dot_general(h_ref[:, slots:], down_sh_ref[...], turn, preferred_element_type=f32)


def mix_kernel(cap, n_z, n_y, experts, at_ref, rank_ref, mix_ref, shared_ref, *refs):
    parts, out_ref = refs[:-1], refs[-1]
    rank = rank_ref[...].astype(bf)
    high = mix_ref[...].astype(bf)
    low = (mix_ref[...] - high.astype(f32)).astype(bf)
    count = rank.shape[0]
    total = shared_ref[...]
    chunk = parts[0].shape[0]
    number = slot_number((count, chunk), 1, cap)
    for i, part_ref in enumerate(parts):
        owner = slot_match(at_ref, chunk, experts, cap, n_z, n_y, i * chunk, 1)
        pick = jnp.dot(rank, owner, preferred_element_type=f32) == number
        part = part_ref[...]
        for w in (high, low):
            weight = jnp.dot(w, owner, preferred_element_type=f32)
            weight = jnp.where(pick, weight, 0.0).astype(bf)
            total += jnp.dot(weight, part, preferred_element_type=f32)
    out_ref[...] = total.astype(bf)


def turned_by(value, axis, d):
    n = lax.axis_size(axis)
    return lax.ppermute(value, axis, [(i, (i + d) % n) for i in range(n)]) if d % n else value


def crossed_with(value, axis, bit):
    return lax.ppermute(value, axis, [(i, i ^ bit) for i in range(lax.axis_size(axis))])


def over_z(value, shift, back=False):
    n_gr, n_z, n_y = lax.axis_size("gr"), lax.axis_size("zl"), lax.axis_size("y")
    n = n_gr * n_z
    pairs = [(z * n_y + y, (z + shift(y)) % n * n_y + y) for z in range(n) for y in range(n_y)]
    return lax.ppermute(value, GF, [p[::-1] for p in pairs] if back else pairs)


def back_along_z(value, z_off):
    n_z = lax.axis_size("zl")
    if z_off == 0:
        return value
    return over_z(
        value,
        lambda y: z_off if 2 * z_off < n_z or (2 * z_off == n_z and y % 2 == 0) else z_off - n_z,
        True,
    )


def from_all_z(block, weights):
    n_z = lax.axis_size("zl")
    ahead, behind = [block], [block]
    for _ in range(n_z // 2 - 1):
        ahead.append(over_z(ahead[-1], lambda y: 1))
        behind.append(over_z(behind[-1], lambda y: -1))
    even = lax.axis_index("y") % 2 == 0
    far = over_z(jnp.where(even, ahead[-1], behind[-1]), lambda y: 1 if y % 2 == 0 else -1)
    return lax.optimization_barrier((ahead + [far] + behind[:0:-1], weights))


def from_all_x(value, beside=()):
    n_x = lax.axis_size("x")
    if n_x != 4:
        return [turned_by(value, "x", n_x - j) for j in range(n_x)], beside
    half = value.shape[0] // 2
    left, right = turned_by(value, "x", 1), turned_by(value, "x", 3)
    left, right, beside = lax.optimization_barrier((left, right, beside))
    far = [turned_by(left[:half], "x", 1), turned_by(right[half:], "x", 3)]
    return [value, right, jnp.concatenate(far, axis=0), left], beside


def on_device(tokens, routes, route_weight, norm_gain, gate_experts, up_experts, down_experts,
              gate_shared, up_shared, down_shared):
    n_gr, n_fs, n_tp = lax.axis_size("gr"), lax.axis_size(FS), lax.axis_size(TP)
    n_z, n_y, n_x = lax.axis_size("zl"), lax.axis_size("y"), lax.axis_size("x")
    fs_at, tp_at, x_at, core = lax.axis_index(FS), lax.axis_index(TP), lax.axis_index("x"), lax.axis_index("core")
    at = jnp.stack([tp_at, lax.axis_index("zl"), lax.axis_index("y"), x_at, core]).astype(jnp.int32)
    per_group, rows_here, cols = gate_experts.shape[1:]
    count, top = routes.shape
    width = tokens.shape[1]
    experts = per_group * n_gr
    cap = (3 * count * top + 2 * experts - 1) // (2 * experts)
    slots = experts * cap
    block_rows = n_gr * cap

    in_smem, in_vmem = pl.BlockSpec(memory_space=pltpu.SMEM), pl.BlockSpec(memory_space=pltpu.VMEM)
    vmem = pltpu.CompilerParams(vmem_limit_bytes=48 * 1024 * 1024)
    sh_rows, sh_cols = gate_shared.shape
    half = sh_rows * 2 * sh_cols // cols
    times = sh_rows // half
    gain_sh = lax.dynamic_slice_in_dim(norm_gain, fs_at * sh_rows, sh_rows, 0)[:, None]
    ride = half + down_shared.shape[0]
    normed, rank, mix, block = pl.pallas_call(
        pack_kernel,
        out_shape=(
            jax.ShapeDtypeStruct((count, width), bf),
            jax.ShapeDtypeStruct((count, experts), f32),
            jax.ShapeDtypeStruct((count, experts), f32),
            jax.ShapeDtypeStruct((count + ride + top, cols), bf),
        ),
        in_specs=[in_smem] + [in_vmem] * 7,
        out_specs=(in_vmem,) * 4,
        compiler_params=vmem,
        name="pack",
    )(at, tokens, routes, route_weight, gate_shared, up_shared, gain_sh, down_shared)
    gain = lax.dynamic_slice_in_dim(norm_gain, tp_at * cols, cols, 0)
    weights = [(gate_experts[0] * gain).astype(bf), (up_experts[0] * gain).astype(bf), down_experts[0].astype(bf)]
    weights = jnp.stack(weights, axis=1)
    weights = jnp.broadcast_to(weights[None], (n_gr, *weights.shape)).reshape(-1, 3, rows_here, cols)
    with jax.named_scope("zchain"):
        blocks, weights = from_all_z(block, weights)
    *chosen, ridden = pl.pallas_call(
        functools.partial(select_kernel, cap, n_gr, n_y, count, top),
        out_shape=(jax.ShapeDtypeStruct((slots // n_y, cols), bf),) * n_y
        + (jax.ShapeDtypeStruct((n_z, ride, cols), bf),),
        in_specs=[in_smem] + [in_vmem] * n_z,
        out_specs=(in_vmem,) * (n_y + 1),
        compiler_params=vmem,
        name="select",
    )(at, *blocks)
    with jax.named_scope("yturn"):
        reached = [turned_by(chosen[y], "y", y) for y in range(n_y)]

    with jax.named_scope("weights"):
        weights = lax.all_to_all(weights, GF, split_axis=0, concat_axis=0, tiled=True)
    down_w = weights[:, 2].reshape(n_gr, n_fs * rows_here, cols)

    ridden, reached = lax.optimization_barrier((ridden, reached))
    ridden = [turned_by(ridden, "y", n_y - y) for y in range(n_y)]
    rows_mine, ridden = from_all_x(jnp.concatenate(reached, axis=0), ridden)
    rows_other = [crossed_with(r, "core", 1) for r in rows_mine]

    near = n_fs // n_tp
    units = near * rows_here
    both = weights.reshape(n_gr, n_tp, near, 3, rows_here, cols)[:, :, :, :2].transpose(1, 0, 2, 3, 4, 5)
    with jax.named_scope("columns"):
        both = lax.all_to_all(both, TP, split_axis=0, concat_axis=0, tiled=True)

    gate_sw, up_sw, down_sw, shared_hidden = pl.pallas_call(
        functools.partial(shared_kernel, half, times),
        out_shape=(
            jax.ShapeDtypeStruct((width, sh_cols), bf),
            jax.ShapeDtypeStruct((width, sh_cols), bf),
            jax.ShapeDtypeStruct((n_fs * down_shared.shape[0], cols), bf),
            jax.ShapeDtypeStruct((sh_cols, count), bf),
        ),
        in_specs=[in_smem] + [in_vmem] * (1 + n_y),
        out_specs=(in_vmem,) * 4,
        scratch_shapes=[pltpu.VMEM((width, 2 * sh_cols), bf)],
        compiler_params=vmem,
        cost_estimate=pl.CostEstimate(
            flops=4 * count * width * sh_cols, bytes_accessed=4 * width * count, transcendentals=0
        ),
        name="shared",
    )(at, normed, *ridden)

    row_block = slots // 6
    whole = pl.BlockSpec((n_gr, units, width), lambda i: (0, 0, 0))
    hidden, gate_w, up_w = pl.pallas_call(
        functools.partial(hidden_kernel, cap, n_gr),
        out_shape=(
            jax.ShapeDtypeStruct((units, slots + count), bf),
            jax.ShapeDtypeStruct((n_gr, units, width), bf),
            jax.ShapeDtypeStruct((n_gr, units, width), bf),
        ),
        grid=(slots // row_block,),
        in_specs=[in_smem, in_vmem, in_vmem] + [pl.BlockSpec((row_block, cols), lambda i: (i, 0))] * n_tp,
        out_specs=(pl.BlockSpec((units, slots + count), lambda i: (0, 0)), whole, whole),
        scratch_shapes=[pltpu.VMEM((2 * n_gr * units, width), bf)],
        compiler_params=vmem,
        cost_estimate=pl.CostEstimate(
            flops=4 * n_gr * units * slots * width, bytes_accessed=2 * slots * width, transcendentals=units * slots
        ),
        name="gate_up",
    )(at, shared_hidden, both, *rows_mine, *rows_other)

    mine = [turned_by(hidden, "x", n_x - j) for j in range(n_x)]
    others = [crossed_with(h, "core", 1) for h in mine]
    *picked, shared = pl.pallas_call(
        functools.partial(down_kernel, cap, n_gr, n_y),
        out_shape=(jax.ShapeDtypeStruct((slots // n_y, cols), bf),) * n_y
        + (jax.ShapeDtypeStruct((count, cols), f32),),
        in_specs=[in_smem] + [in_vmem] * (2 + n_tp),
        out_specs=(in_vmem,) * (n_y + 1),
        scratch_shapes=[pltpu.VMEM((n_tp * units, slots + count), bf)],
        compiler_params=vmem,
        cost_estimate=pl.CostEstimate(
            flops=2 * n_gr * slots * n_tp * units * cols, bytes_accessed=2 * slots * n_tp * units, transcendentals=0
        ),
        name="down",
    )(at, down_w, down_sw, *mine, *others)
    picked = [turned_by(picked[y], "y", n_y - y) for y in range(n_y)]
    returned = []
    for z in range(n_z):
        part = jnp.concatenate([p[z * block_rows : (z + 1) * block_rows] for p in picked], axis=0)
        returned.append(back_along_z(part, z))
    mixed = pl.pallas_call(
        functools.partial(mix_kernel, cap, n_z, n_y, experts),
        out_shape=jax.ShapeDtypeStruct((count, cols), bf),
        in_specs=[in_smem] + [in_vmem] * (3 + n_z),
        out_specs=in_vmem,
        compiler_params=vmem,
        name="mix",
    )(at, rank, mix, shared, *returned)
    return (mixed, gate_w[:, None], up_w[:, None], down_w[:, None], gate_sw, up_sw, down_sw)


def solution(mesh):
    gr, fs, tp = mesh.devices.shape
    n_y = 4 if fs % 4 == 0 else 1
    fine = Mesh(mesh.devices.reshape(gr, fs // n_y, n_y, tp // 2, 2), ("gr", "zl", "y", "x", "core"))
    return jax.shard_map(
        on_device,
        mesh=fine,
        in_specs=(
            P(GF, None),
            P(GF, None),
            P(GF, None),
            P(),
            P("gr", None, FS, TP),
            P("gr", None, FS, TP),
            P("gr", None, FS, TP),
            P(FS, TP),
            P(FS, TP),
            P(FS, TP),
        ),
        out_specs=(
            P(GF, TP),
            P(None, FS, TP, None),
            P(None, FS, TP, None),
            P(None, FS, None, TP),
            P(None, TP),
            P(None, TP),
            P(None, TP),
        ),
        check_vma=False,
    )
```

```python
import functools


import jax
import jax.numpy as jnp
from jax import lax
from jax.experimental import pallas as pl
from jax.experimental.pallas import tpu as pltpu
from jax.sharding import Mesh, PartitionSpec as P

EPS = 1e-06
bf = jnp.bfloat16
f32 = jnp.float32
FS = ("zl", "y")
TP = ("x", "core")
GF = ("gr", "zl", "y")


def slot_number(shape, dim, cap):
    return lax.rem(lax.broadcasted_iota(jnp.int32, shape, dim), cap).astype(f32)


def pack_kernel(at_ref, tok_ref, route_ref, weight_ref, gate_ref, up_ref, gain_ref, down_ref,
                normed_ref, block_ref):
    cols = block_ref.shape[1]
    values = tok_ref[...].astype(f32)
    scale = lax.rsqrt(jnp.mean(values * values, axis=-1, keepdims=True) + EPS)
    normed_ref[...] = (values * scale).astype(bf)
    count, top = route_ref.shape
    block_ref[:count, :] = normed_ref[:, pl.ds(pl.multiple_of(at_ref[0] * cols, cols), cols)]
    rows, units = gate_ref.shape
    gate = (gate_ref[...] * gain_ref[...]).astype(bf)
    up = (up_ref[...] * gain_ref[...]).astype(bf)
    times = cols // (2 * units)
    half = rows // times
    parts = []
    for i in range(times):
        parts += [gate[i * half : (i + 1) * half], up[i * half : (i + 1) * half]]
    block_ref[count : count + half, :] = jnp.concatenate(parts, axis=1)
    below = count + half + down_ref.shape[0]
    block_ref[count + half : below, :] = down_ref[...].astype(bf)
    lane = lax.broadcasted_iota(jnp.int32, (cols, 128), 1)

    def turned(value):
        value = jnp.concatenate([value, jnp.zeros((cols - count, top), f32)], axis=0)
        wide = jnp.zeros((cols, 128), f32)
        for j in range(top):
            wide = jnp.where(lane == j, value[:, j : j + 1], wide)
        return wide.T[:top]

    block_ref[below : below + top, :] = turned(route_ref[...].astype(f32)).astype(bf)
    weight = turned(weight_ref[...])
    high = weight.astype(bf)
    block_ref[below + top : below + 2 * top, :] = high
    block_ref[below + 2 * top :, :] = (weight - high.astype(f32)).astype(bf)


def slots_here(cap, n_gr, n_y, n_z, count, top, at_ref):
    here = n_y * n_gr
    rows = here * cap
    row = lax.broadcasted_iota(jnp.int32, (count, count), 0)
    col = lax.broadcasted_iota(jnp.int32, (count, count), 1)
    before = jnp.where(row < col, 1.0, 0.0).astype(bf)
    r = lax.broadcasted_iota(jnp.int32, (here, count), 0)
    y = lax.rem(lax.div(r, n_gr) + at_ref[2], n_y)
    expert = (lax.rem(r, n_gr) * n_z * n_y + at_ref[1] * n_y + y).astype(f32)
    q = lax.broadcasted_iota(jnp.int32, (rows, here), 0)
    first = cap * lax.broadcasted_iota(jnp.int32, (rows, here), 1)
    owner = jnp.where((q >= first) & (q < first + cap), 1.0, 0.0).astype(bf)
    number = slot_number((rows, count), 0, cap)

    def of(block_ref):
        last = block_ref.shape[0] - 3 * top
        routes = block_ref[last : last + top, :count].astype(f32)
        hits = [routes[j : j + 1, :] == expert for j in range(top)]
        chosen = jnp.zeros((here, count), f32)
        for hit in hits:
            chosen = jnp.where(hit, 1.0, chosen)
        rank = jnp.dot(chosen.astype(bf), before, preferred_element_type=f32)
        rank = jnp.where(chosen > 0, rank, -1.0).astype(bf)
        return hits, jnp.dot(owner, rank, preferred_element_type=f32) == number

    return owner, of


def select_kernel(cap, n_gr, n_y, count, top, at_ref, *refs):
    n_z = len(refs) - n_y - 1
    blocks, outs, shared_ref = refs[:n_z], refs[n_z:-1], refs[-1]
    _, of = slots_here(cap, n_gr, n_y, n_z, count, top, at_ref)
    each = n_gr * cap
    for i in range(n_z):
        block_ref = blocks[i]
        _, pick = of(block_ref)
        pick = jnp.where(pick, 1.0, 0.0).astype(bf)
        picked = jnp.dot(pick, block_ref[:count, :], preferred_element_type=f32).astype(bf)
        for y_off in range(n_y):
            outs[y_off][i * each : (i + 1) * each, :] = picked[y_off * each : (y_off + 1) * each]
        shared_ref[i] = block_ref[count : block_ref.shape[0] - 3 * top, :]


def coef_kernel(cap, n_gr, n_y, count, top, at_ref, *refs):
    blocks, out_ref = refs[:-1], refs[-1]
    owner, of = slots_here(cap, n_gr, n_y, len(blocks), count, top, at_ref)
    for i, block_ref in enumerate(blocks):
        hits, pick = of(block_ref)
        for k in range(2):
            first = block_ref.shape[0] - (2 - k) * top
            weight = block_ref[first : first + top, :count].astype(f32)
            mine = jnp.zeros(hits[0].shape, f32)
            for j, hit in enumerate(hits):
                mine = jnp.where(hit, weight[j : j + 1, :], mine)
            spread = jnp.dot(owner, mine.astype(bf), preferred_element_type=f32)
            out_ref[i, k] = jnp.where(pick, spread, 0.0).astype(bf)


def shared_kernel(half, times, at_ref, normed_ref, *refs):
    blocks, (gate_ref, up_ref, down_ref, hidden_ref, pair_ref) = refs[:-5], refs[-5:]
    n_y, n_z = len(blocks), blocks[0].shape[0]
    rows = half * times
    both = pair_ref.shape[1]
    below = blocks[0].shape[1] - half
    for j in range(n_y):
        for i in range(n_z):
            p = lax.rem(at_ref[1] - i + n_z, n_z) * n_y + lax.rem(at_ref[2] + j, n_y)
            for t in range(times):
                first = pl.multiple_of(p * rows + t * half, half)
                pair_ref[pl.ds(first, half), :] = blocks[j][i, :half, t * both : (t + 1) * both]
            down_ref[pl.ds(pl.multiple_of(p * below, below), below), :] = blocks[j][i, half:, :]
    pair = pair_ref[...]
    gate_ref[...] = pair[:, : both // 2]
    up_ref[...] = pair[:, both // 2 :]
    turned = jnp.dot(normed_ref[...], pair, preferred_element_type=f32).T
    gate, up = turned[: both // 2], turned[both // 2 :]
    hidden_ref[...] = (gate / (1.0 + jnp.exp(-gate)) * up).astype(bf)


def hidden_kernel(cap, n_gr, at_ref, shared_ref, both_ref, *refs):
    rows_refs, (out_ref, gate_ref, up_ref, w_ref) = refs[:-4], refs[-4:]
    n_x = len(rows_refs) // 2
    near, rows_here, cols = both_ref.shape[2], both_ref.shape[4], both_ref.shape[5]
    units = near * rows_here
    rows = rows_refs[0].shape[0]

    def lanes_of(c, j):
        core = at_ref[4] if c == 0 else 1 - at_ref[4]
        owner = lax.rem(at_ref[3] + j, n_x) * 2 + core
        return pl.ds(pl.multiple_of(owner * cols, cols), cols)

    @pl.when(pl.program_id(0) == 0)
    def _():
        for p in range(2 * n_x):
            lanes = slice(p * cols, (p + 1) * cols)
            for g in range(n_gr):
                for q in range(near):
                    for mat, served in ((0, gate_ref), (1, up_ref)):
                        piece = both_ref[p, g, q, mat]
                        first = q * rows_here
                        served[g, first : first + rows_here, lanes] = piece
                        first += (2 * g + mat) * units
                        w_ref[first : first + rows_here, lanes] = piece
        out_ref[:, out_ref.shape[1] - shared_ref.shape[1] :] = shared_ref[...]

    total = jnp.zeros((2 * n_gr * units, rows), f32)
    for j in range(n_x):
        for c in range(2):
            w = w_ref[:, lanes_of(c, j)]
            total += lax.dot_general(
                w, rows_refs[c * n_x + j][...], (((1,), (1,)), ((), ())), preferred_element_type=f32
            )
    slot = lax.broadcasted_iota(jnp.int32, (units, rows), 1) + pl.program_id(0) * rows
    group = lax.div(lax.rem(slot, cap * n_gr), cap)
    gate, up = total[:units], total[units : 2 * units]
    for g in range(1, n_gr):
        gate = jnp.where(group == g, total[2 * g * units : (2 * g + 1) * units], gate)
        up = jnp.where(group == g, total[(2 * g + 1) * units : (2 * g + 2) * units], up)
    hidden = (gate / (1.0 + jnp.exp(-gate)) * up).astype(bf)
    out_ref[:, pl.ds(pl.multiple_of(pl.program_id(0) * rows, 128), rows)] = hidden


def down_kernel(cap, n_gr, n_y, at_ref, down_ref, down_sh_ref, *refs):
    pieces, outs, (shared_ref, h_ref) = refs[: -2 - n_y], refs[-2 - n_y : -2], refs[-2:]
    n_x = len(pieces) // 2
    units = pieces[0].shape[0]
    each, cols = outs[0].shape
    for c in range(2):
        core = at_ref[4] if c == 0 else 1 - at_ref[4]
        for j in range(n_x):
            first = (lax.rem(at_ref[3] + j, n_x) * 2 + core) * units
            h_ref[pl.ds(pl.multiple_of(first, units), units), :] = pieces[c * n_x + j][...]
    turn = (((0,), (0,)), ((), ()))
    for pair in range(n_y // 2):
        first = pair * 2 * each
        h = h_ref[:, first : first + 2 * each]
        slot = lax.broadcasted_iota(jnp.int32, (2 * each, cols), 0) + first
        group = lax.div(lax.rem(slot, cap * n_gr), cap)
        picked = lax.dot_general(h, down_ref[0], turn, preferred_element_type=f32)
        for g in range(1, n_gr):
            other = lax.dot_general(h, down_ref[g], turn, preferred_element_type=f32)
            picked = jnp.where(group == g, other, picked)
        picked = picked.astype(bf)
        outs[2 * pair][...] = picked[:each]
        outs[2 * pair + 1][...] = picked[each:]
    slots = n_y * each
    shared_ref[...] = lax.dot_general(h_ref[:, slots:], down_sh_ref[...], turn, preferred_element_type=f32)


def mix_kernel(coef_ref, shared_ref, *refs):
    n_z = coef_ref.shape[0]
    parts, outs = refs[:-n_z], refs[-n_z:]
    turn = (((0,), (0,)), ((), ()))
    each = parts[0].shape[0] // n_z
    for i in range(n_z):
        rows = jnp.concatenate([p[i * each : (i + 1) * each, :] for p in parts], axis=0)
        total = lax.dot_general(coef_ref[i, 0], rows, turn, preferred_element_type=f32)
        total += lax.dot_general(coef_ref[i, 1], rows, turn, preferred_element_type=f32)
        outs[i][...] = total + shared_ref[...] if i == 0 else total


def turned_by(value, axis, d):
    n = lax.axis_size(axis)
    return lax.ppermute(value, axis, [(i, (i + d) % n) for i in range(n)]) if d % n else value


def crossed_with(value, axis, bit):
    return lax.ppermute(value, axis, [(i, i ^ bit) for i in range(lax.axis_size(axis))])


def over_z(value, shift, back=False):
    n_gr, n_z, n_y = lax.axis_size("gr"), lax.axis_size("zl"), lax.axis_size("y")
    n = n_gr * n_z
    pairs = [(z * n_y + y, (z + shift(y)) % n * n_y + y) for z in range(n) for y in range(n_y)]
    return lax.ppermute(value, GF, [p[::-1] for p in pairs] if back else pairs)


def summed_back(parts):
    n_z = lax.axis_size("zl")
    half = n_z // 2
    even = lax.axis_index("y") % 2 == 0
    far = over_z(parts[half].astype(bf), lambda y: 1 if y % 2 else -1)
    lower, upper = jnp.where(even, far, 0).astype(f32), jnp.where(even, 0, far).astype(f32)
    for s in range(half - 1, 0, -1):
        lower = over_z((parts[s] + lower).astype(bf), lambda y: -1).astype(f32)
        upper = over_z((parts[n_z - s] + upper).astype(bf), lambda y: 1).astype(f32)
    return (parts[0] + lower + upper).astype(bf)


def from_all_z(block, weights):
    n_z = lax.axis_size("zl")
    ahead, behind = [block], [block]
    for _ in range(n_z // 2 - 1):
        ahead.append(over_z(ahead[-1], lambda y: 1))
        behind.append(over_z(behind[-1], lambda y: -1))
    even = lax.axis_index("y") % 2 == 0
    far = over_z(jnp.where(even, ahead[-1], behind[-1]), lambda y: 1 if y % 2 == 0 else -1)
    return lax.optimization_barrier((ahead + [far] + behind[:0:-1], weights))


def from_all_x(value, beside=()):
    n_x = lax.axis_size("x")
    if n_x != 4:
        return [turned_by(value, "x", n_x - j) for j in range(n_x)], beside
    half = value.shape[0] // 2
    left, right = turned_by(value, "x", 1), turned_by(value, "x", 3)
    left, right, beside = lax.optimization_barrier((left, right, beside))
    far = [turned_by(left[:half], "x", 1), turned_by(right[half:], "x", 3)]
    return [value, right, jnp.concatenate(far, axis=0), left], beside


def on_device(tokens, routes, route_weight, norm_gain, gate_experts, up_experts, down_experts,
              gate_shared, up_shared, down_shared):
    n_gr, n_fs, n_tp = lax.axis_size("gr"), lax.axis_size(FS), lax.axis_size(TP)
    n_z, n_y, n_x = lax.axis_size("zl"), lax.axis_size("y"), lax.axis_size("x")
    fs_at, tp_at, x_at, core = lax.axis_index(FS), lax.axis_index(TP), lax.axis_index("x"), lax.axis_index("core")
    at = jnp.stack([tp_at, lax.axis_index("zl"), lax.axis_index("y"), x_at, core]).astype(jnp.int32)
    per_group, rows_here, cols = gate_experts.shape[1:]
    count, top = routes.shape
    width = tokens.shape[1]
    experts = per_group * n_gr
    cap = (3 * count * top + 2 * experts - 1) // (2 * experts)
    slots = experts * cap
    block_rows = n_gr * cap

    in_smem, in_vmem = pl.BlockSpec(memory_space=pltpu.SMEM), pl.BlockSpec(memory_space=pltpu.VMEM)
    vmem = pltpu.CompilerParams(vmem_limit_bytes=48 * 1024 * 1024)
    sh_rows, sh_cols = gate_shared.shape
    half = sh_rows * 2 * sh_cols // cols
    times = sh_rows // half
    gain_sh = lax.dynamic_slice_in_dim(norm_gain, fs_at * sh_rows, sh_rows, 0)[:, None]
    ride = half + down_shared.shape[0]
    normed, block = pl.pallas_call(
        pack_kernel,
        out_shape=(
            jax.ShapeDtypeStruct((count, width), bf),
            jax.ShapeDtypeStruct((count + ride + 3 * top, cols), bf),
        ),
        in_specs=[in_smem] + [in_vmem] * 7,
        out_specs=(in_vmem,) * 2,
        compiler_params=vmem,
        name="pack",
    )(at, tokens, routes, route_weight, gate_shared, up_shared, gain_sh, down_shared)
    gain = lax.dynamic_slice_in_dim(norm_gain, tp_at * cols, cols, 0)
    weights = [(gate_experts[0] * gain).astype(bf), (up_experts[0] * gain).astype(bf), down_experts[0].astype(bf)]
    weights = jnp.stack(weights, axis=1)
    weights = jnp.broadcast_to(weights[None], (n_gr, *weights.shape)).reshape(-1, 3, rows_here, cols)
    blocks, weights = from_all_z(block, weights)
    *chosen, ridden = pl.pallas_call(
        functools.partial(select_kernel, cap, n_gr, n_y, count, top),
        out_shape=(jax.ShapeDtypeStruct((slots // n_y, cols), bf),) * n_y
        + (jax.ShapeDtypeStruct((n_z, ride, cols), bf),),
        in_specs=[in_smem] + [in_vmem] * n_z,
        out_specs=(in_vmem,) * (n_y + 1),
        compiler_params=vmem,
        name="select",
    )(at, *blocks)
    coef = pl.pallas_call(
        functools.partial(coef_kernel, cap, n_gr, n_y, count, top),
        out_shape=jax.ShapeDtypeStruct((n_z, 2, n_y * block_rows, count), bf),
        in_specs=[in_smem] + [in_vmem] * n_z,
        out_specs=in_vmem,
        compiler_params=vmem,
        cost_estimate=pl.CostEstimate(flops=2**30, bytes_accessed=2**21, transcendentals=0),
        name="coef",
    )(at, *blocks)
    reached = [turned_by(chosen[y], "y", y) for y in range(n_y)]

    weights = lax.all_to_all(weights, GF, split_axis=0, concat_axis=0, tiled=True)
    down_w = weights[:, 2].reshape(n_gr, n_fs * rows_here, cols)

    ridden, reached = lax.optimization_barrier((ridden, reached))
    ridden = [turned_by(ridden, "y", n_y - y) for y in range(n_y)]
    rows_mine, ridden = from_all_x(jnp.concatenate(reached, axis=0), ridden)
    rows_other = [crossed_with(r, "core", 1) for r in rows_mine]

    near = n_fs // n_tp
    units = near * rows_here
    both = weights.reshape(n_gr, n_tp, near, 3, rows_here, cols)[:, :, :, :2].transpose(1, 0, 2, 3, 4, 5)
    both = lax.all_to_all(both, TP, split_axis=0, concat_axis=0, tiled=True)

    gate_sw, up_sw, down_sw, shared_hidden = pl.pallas_call(
        functools.partial(shared_kernel, half, times),
        out_shape=(
            jax.ShapeDtypeStruct((width, sh_cols), bf),
            jax.ShapeDtypeStruct((width, sh_cols), bf),
            jax.ShapeDtypeStruct((n_fs * down_shared.shape[0], cols), bf),
            jax.ShapeDtypeStruct((sh_cols, count), bf),
        ),
        in_specs=[in_smem] + [in_vmem] * (1 + n_y),
        out_specs=(in_vmem,) * 4,
        scratch_shapes=[pltpu.VMEM((width, 2 * sh_cols), bf)],
        compiler_params=vmem,
        cost_estimate=pl.CostEstimate(
            flops=4 * count * width * sh_cols, bytes_accessed=4 * width * count, transcendentals=0
        ),
        name="shared",
    )(at, normed, *ridden)

    row_block = slots // 6
    whole = pl.BlockSpec((n_gr, units, width), lambda i: (0, 0, 0))
    hidden, gate_w, up_w = pl.pallas_call(
        functools.partial(hidden_kernel, cap, n_gr),
        out_shape=(
            jax.ShapeDtypeStruct((units, slots + count), bf),
            jax.ShapeDtypeStruct((n_gr, units, width), bf),
            jax.ShapeDtypeStruct((n_gr, units, width), bf),
        ),
        grid=(slots // row_block,),
        in_specs=[in_smem, in_vmem, in_vmem] + [pl.BlockSpec((row_block, cols), lambda i: (i, 0))] * n_tp,
        out_specs=(pl.BlockSpec((units, slots + count), lambda i: (0, 0)), whole, whole),
        scratch_shapes=[pltpu.VMEM((2 * n_gr * units, width), bf)],
        compiler_params=vmem,
        cost_estimate=pl.CostEstimate(
            flops=4 * n_gr * units * slots * width, bytes_accessed=2 * slots * width, transcendentals=units * slots
        ),
        name="gate_up",
    )(at, shared_hidden, both, *rows_mine, *rows_other)

    mine = [turned_by(hidden, "x", n_x - j) for j in range(n_x)]
    others = [crossed_with(h, "core", 1) for h in mine]
    *picked, shared = pl.pallas_call(
        functools.partial(down_kernel, cap, n_gr, n_y),
        out_shape=(jax.ShapeDtypeStruct((slots // n_y, cols), bf),) * n_y
        + (jax.ShapeDtypeStruct((count, cols), f32),),
        in_specs=[in_smem] + [in_vmem] * (2 + n_tp),
        out_specs=(in_vmem,) * (n_y + 1),
        scratch_shapes=[pltpu.VMEM((n_tp * units, slots + count), bf)],
        compiler_params=vmem,
        cost_estimate=pl.CostEstimate(
            flops=2 * n_gr * slots * n_tp * units * cols, bytes_accessed=2 * slots * n_tp * units, transcendentals=0
        ),
        name="down",
    )(at, down_w, down_sw, *mine, *others)
    picked = [turned_by(picked[y], "y", n_y - y) for y in range(n_y)]
    parts = pl.pallas_call(
        mix_kernel,
        out_shape=(jax.ShapeDtypeStruct((count, cols), f32),) * n_z,
        in_specs=[in_vmem] * (2 + n_y),
        out_specs=(in_vmem,) * n_z,
        compiler_params=vmem,
        name="mix",
    )(coef, shared, *picked)
    mixed = summed_back(parts)
    return (mixed, gate_w[:, None], up_w[:, None], down_w[:, None], gate_sw, up_sw, down_sw)


def solution(mesh):
    gr, fs, tp = mesh.devices.shape
    n_y = 4 if fs % 4 == 0 else 1
    fine = Mesh(mesh.devices.reshape(gr, fs // n_y, n_y, tp // 2, 2), ("gr", "zl", "y", "x", "core"))

    return jax.shard_map(
        on_device,
        mesh=fine,
        in_specs=(
            P(GF, None),
            P(GF, None),
            P(GF, None),
            P(),
            P("gr", None, FS, TP),
            P("gr", None, FS, TP),
            P("gr", None, FS, TP),
            P(FS, TP),
            P(FS, TP),
            P(FS, TP),
        ),
        out_specs=(
            P(GF, TP),
            P(None, FS, TP, None),
            P(None, FS, TP, None),
            P(None, FS, None, TP),
            P(None, TP),
            P(None, TP),
            P(None, TP),
        ),
        check_vma=False,
    )
```

```python
import functools


import jax
import jax.numpy as jnp
from jax import lax
from jax.experimental import pallas as pl
from jax.experimental.pallas import tpu as pltpu
from jax.sharding import Mesh, PartitionSpec as P

EPS = 1e-06
bf = jnp.bfloat16
f32 = jnp.float32
FS = ("zl", "y")
TP = ("x", "core")
GF = ("gr", "zl", "y")


def slot_number(shape, dim, cap):
    return lax.rem(lax.broadcasted_iota(jnp.int32, shape, dim), cap).astype(f32)


def norm(tokens):
    values = tokens.astype(f32)
    return (values * lax.rsqrt(jnp.mean(values * values, axis=-1, keepdims=True) + EPS)).astype(bf)


def pack_kernel(at_ref, gain_ref, *refs):
    sources, block_ref, held, normed_ref, sems = refs[:6], refs[6], refs[7:13], refs[13], refs[14]
    copies = [pltpu.make_async_copy(source, to, sems.at[i]) for i, (source, to) in enumerate(zip(sources, held))]
    for copy in copies:
        copy.start()
    for copy in copies:
        copy.wait()
    tok_ref, route_ref, weight_ref, gate_ref, up_ref, down_ref = held
    cols = block_ref.shape[1]
    normed_ref[...] = norm(tok_ref[...])
    top, count = route_ref.shape
    block_ref[:count, :] = normed_ref[:, pl.ds(pl.multiple_of(at_ref[0] * cols, cols), cols)]
    rows, units = gate_ref.shape
    gate = (gate_ref[...] * gain_ref[...]).astype(bf)
    up = (up_ref[...] * gain_ref[...]).astype(bf)
    times = cols // (2 * units)
    half = rows // times
    parts = []
    for i in range(times):
        parts += [gate[i * half : (i + 1) * half], up[i * half : (i + 1) * half]]
    block_ref[count : count + half, :] = jnp.concatenate(parts, axis=1)
    below = count + half + down_ref.shape[0]
    block_ref[count + half : below, :] = down_ref[...].astype(bf)
    block_ref[below:, :] = jnp.zeros((3 * top, cols), bf)
    weight = weight_ref[...]
    high = weight.astype(bf)
    block_ref[below : below + top, :count] = route_ref[...].astype(f32).astype(bf)
    block_ref[below + top : below + 2 * top, :count] = high
    block_ref[below + 2 * top :, :count] = (weight - high.astype(f32)).astype(bf)


def slots_here(cap, n_gr, n_y, n_z, count, top, at_ref):
    here = n_y * n_gr
    rows = here * cap
    row = lax.broadcasted_iota(jnp.int32, (count, count), 0)
    col = lax.broadcasted_iota(jnp.int32, (count, count), 1)
    before = jnp.where(row < col, 1.0, 0.0).astype(bf)
    r = lax.broadcasted_iota(jnp.int32, (here, count), 0)
    y = lax.rem(lax.div(r, n_gr) + at_ref[2], n_y)
    expert = (lax.rem(r, n_gr) * n_z * n_y + at_ref[1] * n_y + y).astype(f32)
    q = lax.broadcasted_iota(jnp.int32, (rows, here), 0)
    first = cap * lax.broadcasted_iota(jnp.int32, (rows, here), 1)
    owner = jnp.where((q >= first) & (q < first + cap), 1.0, 0.0).astype(bf)
    number = slot_number((rows, count), 0, cap)

    def of(block_ref):
        last = block_ref.shape[0] - 3 * top
        routes = block_ref[last : last + top, :count].astype(f32)
        hits = [routes[j : j + 1, :] == expert for j in range(top)]
        chosen = jnp.zeros((here, count), f32)
        for hit in hits:
            chosen = jnp.where(hit, 1.0, chosen)
        rank = jnp.dot(chosen.astype(bf), before, preferred_element_type=f32)
        rank = jnp.where(chosen > 0, rank, -1.0).astype(bf)
        return hits, jnp.dot(owner, rank, preferred_element_type=f32) == number

    return owner, of


def select_kernel(cap, n_gr, n_y, count, top, at_ref, *refs):
    n_z = len(refs) - n_y - 1
    blocks, outs, shared_ref = refs[:n_z], refs[n_z:-1], refs[-1]
    _, of = slots_here(cap, n_gr, n_y, n_z, count, top, at_ref)
    each = n_gr * cap
    for i in range(n_z):
        block_ref = blocks[i]
        _, pick = of(block_ref)
        pick = jnp.where(pick, 1.0, 0.0).astype(bf)
        picked = jnp.dot(pick, block_ref[:count, :], preferred_element_type=f32).astype(bf)
        for y_off in range(n_y):
            outs[y_off][i * each : (i + 1) * each, :] = picked[y_off * each : (y_off + 1) * each]
        shared_ref[i] = block_ref[count : block_ref.shape[0] - 3 * top, :]


def coef_kernel(cap, n_gr, n_y, count, top, at_ref, *refs):
    blocks, out_ref = refs[:-1], refs[-1]
    owner, of = slots_here(cap, n_gr, n_y, len(blocks), count, top, at_ref)
    for i, block_ref in enumerate(blocks):
        hits, pick = of(block_ref)
        for k in range(2):
            first = block_ref.shape[0] - (2 - k) * top
            weight = block_ref[first : first + top, :count].astype(f32)
            mine = jnp.zeros(hits[0].shape, f32)
            for j, hit in enumerate(hits):
                mine = jnp.where(hit, weight[j : j + 1, :], mine)
            spread = jnp.dot(owner, mine.astype(bf), preferred_element_type=f32)
            out_ref[i, k] = jnp.where(pick, spread, 0.0).astype(bf)


def shared_kernel(half, times, at_ref, tok_ref, *refs):
    blocks, (gate_ref, up_ref, down_ref, hidden_ref, pair_ref) = refs[:-5], refs[-5:]
    n_y, n_z = len(blocks), blocks[0].shape[0]
    rows = half * times
    both = pair_ref.shape[1]
    below = blocks[0].shape[1] - half
    for j in range(n_y):
        for i in range(n_z):
            p = lax.rem(at_ref[1] - i + n_z, n_z) * n_y + lax.rem(at_ref[2] + j, n_y)
            for t in range(times):
                first = pl.multiple_of(p * rows + t * half, half)
                pair_ref[pl.ds(first, half), :] = blocks[j][i, :half, t * both : (t + 1) * both]
            down_ref[pl.ds(pl.multiple_of(p * below, below), below), :] = blocks[j][i, half:, :]
    pair = pair_ref[...]
    gate_ref[...] = pair[:, : both // 2]
    up_ref[...] = pair[:, both // 2 :]
    turned = jnp.dot(norm(tok_ref[...]), pair, preferred_element_type=f32).T
    gate, up = turned[: both // 2], turned[both // 2 :]
    hidden_ref[...] = (gate / (1.0 + jnp.exp(-gate)) * up).astype(bf)


def hidden_kernel(cap, n_gr, at_ref, shared_ref, both_ref, *refs):
    rows_refs, (out_ref, gate_ref, up_ref, w_ref) = refs[:-4], refs[-4:]
    n_x = len(rows_refs) // 2
    near, rows_here, cols = both_ref.shape[2], both_ref.shape[4], both_ref.shape[5]
    units = near * rows_here
    rows = rows_refs[0].shape[0]

    def lanes_of(c, j):
        core = at_ref[4] if c == 0 else 1 - at_ref[4]
        owner = lax.rem(at_ref[3] + j, n_x) * 2 + core
        return pl.ds(pl.multiple_of(owner * cols, cols), cols)

    @pl.when(pl.program_id(0) == 0)
    def _():
        for p in range(2 * n_x):
            lanes = slice(p * cols, (p + 1) * cols)
            for g in range(n_gr):
                for q in range(near):
                    for mat, served in ((0, gate_ref), (1, up_ref)):
                        piece = both_ref[p, g, q, mat]
                        first = q * rows_here
                        served[g, first : first + rows_here, lanes] = piece
                        first += (2 * g + mat) * units
                        w_ref[first : first + rows_here, lanes] = piece
        out_ref[:, out_ref.shape[1] - shared_ref.shape[1] :] = shared_ref[...]

    total = jnp.zeros((2 * n_gr * units, rows), f32)
    for j in range(n_x):
        for c in range(2):
            w = w_ref[:, lanes_of(c, j)]
            total += lax.dot_general(
                w, rows_refs[c * n_x + j][...], (((1,), (1,)), ((), ())), preferred_element_type=f32
            )
    slot = lax.broadcasted_iota(jnp.int32, (units, rows), 1) + pl.program_id(0) * rows
    group = lax.div(lax.rem(slot, cap * n_gr), cap)
    gate, up = total[:units], total[units : 2 * units]
    for g in range(1, n_gr):
        gate = jnp.where(group == g, total[2 * g * units : (2 * g + 1) * units], gate)
        up = jnp.where(group == g, total[(2 * g + 1) * units : (2 * g + 2) * units], up)
    hidden = (gate / (1.0 + jnp.exp(-gate)) * up).astype(bf)
    out_ref[:, pl.ds(pl.multiple_of(pl.program_id(0) * rows, 128), rows)] = hidden


def down_kernel(cap, n_gr, n_y, at_ref, down_ref, down_sh_ref, *refs):
    pieces, outs, (shared_ref, h_ref) = refs[: -2 - n_y], refs[-2 - n_y : -2], refs[-2:]
    n_x = len(pieces) // 2
    units = pieces[0].shape[0]
    each, cols = outs[0].shape
    for c in range(2):
        core = at_ref[4] if c == 0 else 1 - at_ref[4]
        for j in range(n_x):
            first = (lax.rem(at_ref[3] + j, n_x) * 2 + core) * units
            h_ref[pl.ds(pl.multiple_of(first, units), units), :] = pieces[c * n_x + j][...]
    turn = (((0,), (0,)), ((), ()))
    for pair in range(n_y // 2):
        first = pair * 2 * each
        h = h_ref[:, first : first + 2 * each]
        slot = lax.broadcasted_iota(jnp.int32, (2 * each, cols), 0) + first
        group = lax.div(lax.rem(slot, cap * n_gr), cap)
        picked = lax.dot_general(h, down_ref[0], turn, preferred_element_type=f32)
        for g in range(1, n_gr):
            other = lax.dot_general(h, down_ref[g], turn, preferred_element_type=f32)
            picked = jnp.where(group == g, other, picked)
        picked = picked.astype(bf)
        outs[2 * pair][...] = picked[:each]
        outs[2 * pair + 1][...] = picked[each:]
    slots = n_y * each
    shared_ref[...] = lax.dot_general(h_ref[:, slots:], down_sh_ref[...], turn, preferred_element_type=f32)


def mix_kernel(coef_ref, shared_ref, *refs):
    n_z = coef_ref.shape[0]
    parts, outs = refs[:-n_z], refs[-n_z:]
    turn = (((0,), (0,)), ((), ()))
    each = parts[0].shape[0] // n_z
    for i in range(n_z):
        rows = jnp.concatenate([p[i * each : (i + 1) * each, :] for p in parts], axis=0)
        total = lax.dot_general(coef_ref[i, 0], rows, turn, preferred_element_type=f32)
        total += lax.dot_general(coef_ref[i, 1], rows, turn, preferred_element_type=f32)
        outs[i][...] = total + shared_ref[...] if i == 0 else total


def turned_by(value, axis, d):
    n = lax.axis_size(axis)
    return lax.ppermute(value, axis, [(i, (i + d) % n) for i in range(n)]) if d % n else value


def crossed_with(value, axis, bit):
    return lax.ppermute(value, axis, [(i, i ^ bit) for i in range(lax.axis_size(axis))])


def over_z(value, shift, back=False):
    n_gr, n_z, n_y = lax.axis_size("gr"), lax.axis_size("zl"), lax.axis_size("y")
    n = n_gr * n_z
    pairs = [(z * n_y + y, (z + shift(y)) % n * n_y + y) for z in range(n) for y in range(n_y)]
    return lax.ppermute(value, GF, [p[::-1] for p in pairs] if back else pairs)


def summed_back(parts):
    n_z = lax.axis_size("zl")
    half = n_z // 2
    even = lax.axis_index("y") % 2 == 0
    far = over_z(parts[half].astype(bf), lambda y: 1 if y % 2 else -1)
    lower, upper = jnp.where(even, far, 0).astype(f32), jnp.where(even, 0, far).astype(f32)
    for s in range(half - 1, 0, -1):
        lower = over_z((parts[s] + lower).astype(bf), lambda y: -1).astype(f32)
        upper = over_z((parts[n_z - s] + upper).astype(bf), lambda y: 1).astype(f32)
    return (parts[0] + lower + upper).astype(bf)


def from_all_z(block, weights):
    n_z = lax.axis_size("zl")
    ahead, behind = [block], [block]
    for _ in range(n_z // 2 - 1):
        ahead.append(over_z(ahead[-1], lambda y: 1))
        behind.append(over_z(behind[-1], lambda y: -1))
    even = lax.axis_index("y") % 2 == 0
    far = over_z(jnp.where(even, ahead[-1], behind[-1]), lambda y: 1 if y % 2 == 0 else -1)
    return lax.optimization_barrier((ahead + [far] + behind[:0:-1], weights))


def from_all_x(value, beside=()):
    n_x = lax.axis_size("x")
    if n_x != 4:
        return [turned_by(value, "x", n_x - j) for j in range(n_x)], beside
    half = value.shape[0] // 2
    left, right = turned_by(value, "x", 1), turned_by(value, "x", 3)
    left, right, beside = lax.optimization_barrier((left, right, beside))
    far = [turned_by(left[:half], "x", 1), turned_by(right[half:], "x", 3)]
    return [value, right, jnp.concatenate(far, axis=0), left], beside


def on_device(tokens, routes, route_weight, norm_gain, gate_experts, up_experts, down_experts,
              gate_shared, up_shared, down_shared):
    n_gr, n_fs, n_tp = lax.axis_size("gr"), lax.axis_size(FS), lax.axis_size(TP)
    n_z, n_y, n_x = lax.axis_size("zl"), lax.axis_size("y"), lax.axis_size("x")
    fs_at, tp_at, x_at, core = lax.axis_index(FS), lax.axis_index(TP), lax.axis_index("x"), lax.axis_index("core")
    at = jnp.stack([tp_at, lax.axis_index("zl"), lax.axis_index("y"), x_at, core]).astype(jnp.int32)
    per_group, rows_here, cols = gate_experts.shape[1:]
    count, top = routes.shape
    width = tokens.shape[1]
    experts = per_group * n_gr
    cap = (3 * count * top + 2 * experts - 1) // (2 * experts)
    slots = experts * cap
    block_rows = n_gr * cap

    in_smem, in_vmem = pl.BlockSpec(memory_space=pltpu.SMEM), pl.BlockSpec(memory_space=pltpu.VMEM)
    vmem = pltpu.CompilerParams(vmem_limit_bytes=48 * 1024 * 1024)
    sh_rows, sh_cols = gate_shared.shape
    half = sh_rows * 2 * sh_cols // cols
    times = sh_rows // half
    gain_sh = lax.dynamic_slice_in_dim(norm_gain, fs_at * sh_rows, sh_rows, 0)[:, None]
    ride = half + down_shared.shape[0]
    block = pl.pallas_call(
        pack_kernel,
        out_shape=jax.ShapeDtypeStruct((count + ride + 3 * top, cols), bf),
        in_specs=[in_smem, in_vmem] + [pl.BlockSpec(memory_space=pltpu.HBM)] * 6,
        out_specs=in_vmem,
        scratch_shapes=[
            pltpu.VMEM((count, width), bf),
            pltpu.VMEM((top, count), jnp.int32),
            pltpu.VMEM((top, count), f32),
            pltpu.VMEM((sh_rows, sh_cols), f32),
            pltpu.VMEM((sh_rows, sh_cols), f32),
            pltpu.VMEM(down_shared.shape, f32),
            pltpu.VMEM((count, width), bf),
            pltpu.SemaphoreType.DMA((6,)),
        ],
        compiler_params=pltpu.CompilerParams(vmem_limit_bytes=67043328),
        name="pack",
    )(at, gain_sh, tokens, routes.T, route_weight.T, gate_shared, up_shared, down_shared)
    gain = lax.dynamic_slice_in_dim(norm_gain, tp_at * cols, cols, 0)
    weights = [(gate_experts[0] * gain).astype(bf), (up_experts[0] * gain).astype(bf), down_experts[0].astype(bf)]
    weights = jnp.stack(weights, axis=1)
    weights = jnp.broadcast_to(weights[None], (n_gr, *weights.shape)).reshape(-1, 3, rows_here, cols)
    blocks, weights = from_all_z(block, weights)
    *chosen, ridden = pl.pallas_call(
        functools.partial(select_kernel, cap, n_gr, n_y, count, top),
        out_shape=(jax.ShapeDtypeStruct((slots // n_y, cols), bf),) * n_y
        + (jax.ShapeDtypeStruct((n_z, ride, cols), bf),),
        in_specs=[in_smem] + [in_vmem] * n_z,
        out_specs=(in_vmem,) * (n_y + 1),
        compiler_params=vmem,
        name="select",
    )(at, *blocks)
    coef = pl.pallas_call(
        functools.partial(coef_kernel, cap, n_gr, n_y, count, top),
        out_shape=jax.ShapeDtypeStruct((n_z, 2, n_y * block_rows, count), bf),
        in_specs=[in_smem] + [in_vmem] * n_z,
        out_specs=in_vmem,
        compiler_params=vmem,
        cost_estimate=pl.CostEstimate(flops=2**30, bytes_accessed=2**21, transcendentals=0),
        name="coef",
    )(at, *blocks)
    reached = [turned_by(chosen[y], "y", y) for y in range(n_y)]

    weights = lax.all_to_all(weights, GF, split_axis=0, concat_axis=0, tiled=True)
    down_w = weights[:, 2].reshape(n_gr, n_fs * rows_here, cols)

    ridden, reached = lax.optimization_barrier((ridden, reached))
    ridden = [turned_by(ridden, "y", n_y - y) for y in range(n_y)]
    gate_sw, up_sw, down_sw, shared_hidden = pl.pallas_call(
        functools.partial(shared_kernel, half, times),
        out_shape=(
            jax.ShapeDtypeStruct((width, sh_cols), bf),
            jax.ShapeDtypeStruct((width, sh_cols), bf),
            jax.ShapeDtypeStruct((n_fs * down_shared.shape[0], cols), bf),
            jax.ShapeDtypeStruct((sh_cols, count), bf),
        ),
        in_specs=[in_smem] + [in_vmem] * (1 + n_y),
        out_specs=(in_vmem,) * 4,
        scratch_shapes=[pltpu.VMEM((width, 2 * sh_cols), bf)],
        compiler_params=vmem,
        cost_estimate=pl.CostEstimate(
            flops=4 * count * width * sh_cols, bytes_accessed=4 * width * count, transcendentals=0
        ),
        name="shared",
    )(at, tokens, *ridden)
    rows_mine, beside = from_all_x(
        jnp.concatenate(reached, axis=0), (gate_sw, up_sw, down_sw, shared_hidden, coef)
    )
    gate_sw, up_sw, down_sw, shared_hidden, coef = beside
    rows_other = [crossed_with(r, "core", 1) for r in rows_mine]

    near = n_fs // n_tp
    units = near * rows_here
    both = weights.reshape(n_gr, n_tp, near, 3, rows_here, cols)[:, :, :, :2].transpose(1, 0, 2, 3, 4, 5)
    both = lax.all_to_all(both, TP, split_axis=0, concat_axis=0, tiled=True)

    row_block = slots // 6
    whole = pl.BlockSpec((n_gr, units, width), lambda i: (0, 0, 0))
    shared_hidden, down_w = lax.optimization_barrier((shared_hidden, down_w))
    hidden, gate_w, up_w = pl.pallas_call(
        functools.partial(hidden_kernel, cap, n_gr),
        out_shape=(
            jax.ShapeDtypeStruct((units, slots + count), bf),
            jax.ShapeDtypeStruct((n_gr, units, width), bf),
            jax.ShapeDtypeStruct((n_gr, units, width), bf),
        ),
        grid=(slots // row_block,),
        in_specs=[in_smem, in_vmem, in_vmem] + [pl.BlockSpec((row_block, cols), lambda i: (i, 0))] * n_tp,
        out_specs=(pl.BlockSpec((units, slots + count), lambda i: (0, 0)), whole, whole),
        scratch_shapes=[pltpu.VMEM((2 * n_gr * units, width), bf)],
        compiler_params=vmem,
        cost_estimate=pl.CostEstimate(
            flops=4 * n_gr * units * slots * width, bytes_accessed=2 * slots * width, transcendentals=units * slots
        ),
        name="gate_up",
    )(at, shared_hidden, both, *rows_mine, *rows_other)

    mine = [turned_by(hidden, "x", n_x - j) for j in range(n_x)]
    others = [crossed_with(h, "core", 1) for h in mine]
    *picked, shared = pl.pallas_call(
        functools.partial(down_kernel, cap, n_gr, n_y),
        out_shape=(jax.ShapeDtypeStruct((slots // n_y, cols), bf),) * n_y
        + (jax.ShapeDtypeStruct((count, cols), f32),),
        in_specs=[in_smem] + [in_vmem] * (2 + n_tp),
        out_specs=(in_vmem,) * (n_y + 1),
        scratch_shapes=[pltpu.VMEM((n_tp * units, slots + count), bf)],
        compiler_params=vmem,
        cost_estimate=pl.CostEstimate(
            flops=2 * n_gr * slots * n_tp * units * cols, bytes_accessed=2 * slots * n_tp * units, transcendentals=0
        ),
        name="down",
    )(at, down_w, down_sw, *mine, *others)
    picked = [turned_by(picked[y], "y", n_y - y) for y in range(n_y)]
    parts = pl.pallas_call(
        mix_kernel,
        out_shape=(jax.ShapeDtypeStruct((count, cols), f32),) * n_z,
        in_specs=[in_vmem] * (2 + n_y),
        out_specs=(in_vmem,) * n_z,
        compiler_params=vmem,
        name="mix",
    )(coef, shared, *picked)
    mixed = summed_back(parts)
    return (mixed, gate_w[:, None], up_w[:, None], down_w[:, None], gate_sw, up_sw, down_sw)


def solution(mesh):
    gr, fs, tp = mesh.devices.shape
    n_y = 4 if fs % 4 == 0 else 1
    fine = Mesh(mesh.devices.reshape(gr, fs // n_y, n_y, tp // 2, 2), ("gr", "zl", "y", "x", "core"))

    return jax.shard_map(
        on_device,
        mesh=fine,
        in_specs=(
            P(GF, None),
            P(GF, None),
            P(GF, None),
            P(),
            P("gr", None, FS, TP),
            P("gr", None, FS, TP),
            P("gr", None, FS, TP),
            P(FS, TP),
            P(FS, TP),
            P(FS, TP),
        ),
        out_specs=(
            P(GF, TP),
            P(None, FS, TP, None),
            P(None, FS, TP, None),
            P(None, FS, None, TP),
            P(None, TP),
            P(None, TP),
            P(None, TP),
        ),
        check_vma=False,
    )
```
